256 devices in a mesh: sp: 64 (over z, y, core), tp: 4 (over x).
Axes of the slice: x: 4, y: 4, z: 8, core: 2. Of those that a mesh axis runs over, the one named last changes fastest.
Arguments:
- query: bfloat16 [16384, 1536], P('sp', 'tp'), may hold values from -6 to 6
- forget_preact: bfloat16 [16384, 1536], P('sp', 'tp'), may hold values from -6 to 6
- value_input: bfloat16 [16384, 1536], P('sp', 'tp'), may hold values from -6 to 6
- output_gate: bfloat16 [16384, 1536], P('sp', 'tp'), may hold values from -6 to 6
- forget_minimum: float32 [1536], P('tp'), may hold values from 0.88 to 1
- extra_log_decay: float32 [12, 16384], P('tp', 'sp'), may hold values from -0.7 to 0
- head_norm_gain: float32 [1536], P('tp'), may hold values from 0.1 to 1.9
- output_weight: bfloat16 [1536, 3072], P(None, 'tp'), may hold values from -0.15625 to 0.15625
- stream: bfloat16 [16384, 3072], P(('sp', 'tp')), may hold values from -6 to 6
- feedforward_gain: float32 [3072], replicated, may hold values from 0.1 to 1.9
- routes: int32 [16384, 2], P('sp'), may hold values from 0 to 63, all different within a row; in each aligned block of 64 rows (0 to 63, 64 to 127, ...) at most 4 rows name the same one
- router_weight: float32 [16384, 2], P(('sp', 'tp')), may hold values from 0.05 to 1
- expert_gate_weight: bfloat16 [64, 3072, 1024], P('sp', None, 'tp'), may hold values from -0.109375 to 0.109375
- expert_up_weight: bfloat16 [64, 3072, 1024], P('sp', None, 'tp'), may hold values from -0.109375 to 0.109375
- expert_down_weight: bfloat16 [64, 1024, 3072], P('sp', 'tp'), may hold values from -0.1875 to 0.1875
Outputs:
- result: bfloat16 [16384, 3072], P(('sp', 'tp'))
The draws below stay inside these ranges and needn't reach their ends.
Inputs may be any that keep to these rules, and one draw needn't show every extreme that they name: `routes`: each row names 2 different experts; in each aligned block of 64 rows no expert is named by more than 4 rows, a bound that some block reaches.
All inputs are finite; a program needn't handle non-finite values.
Results may differ from the reference program's by a relative error of at most 0.01.
Values may be sent and summed in bfloat16 or wider, within the bound.
No kernel may reach another device: no remote copies, remote signals or barrier semaphores. Data moves between devices by JAX's collectives and lax.ppermute only.
A program may use at most 64 MiB of HBM per device.

```python
import math
import jax
import jax.numpy as jnp
import numpy as np
from jax import lax

D = 3072
HEADS = 12
STATE_ROW_COUNT = 128
VALUE_CHANNELS = 128
FF = 1024
SPAN = 64
TOPK = 2
TOK_DEV = 256
SEQUENCE_TOKENS = 16384
KEY_WIDTH = 1536
VALUE_WIDTH = 1536
EXPERTS = 64
QROWS = 64
CAPQ = 4
N_TP = 4


def draw_forget_preact(key, part):
    base_key, shift_key = jax.random.split(key)
    base_draw = jax.random.normal(base_key, (SEQUENCE_TOKENS, KEY_WIDTH), jnp.float32)
    shift_draw = jax.random.uniform(shift_key, (SEQUENCE_TOKENS // TOK_DEV, 1), jnp.float32, -1.0, 1.0)
    shifted = base_draw + jnp.repeat(shift_draw, TOK_DEV, axis=0)
    return jnp.clip(shifted, -6.0, 6.0).astype(jnp.bfloat16)


def draw_forget_minimum(key, part):
    pick_key, slow_key, fast_key = jax.random.split(key, 3)
    slow_share = 0.5
    slow_head = jax.random.uniform(pick_key, (HEADS, 1), jnp.float32) < slow_share
    slow_rate = jnp.exp(jax.random.uniform(slow_key, (HEADS, STATE_ROW_COUNT), jnp.float32, jnp.log(0.2), jnp.log(2.0))) / SEQUENCE_TOKENS
    fast_rate = jnp.exp(jax.random.uniform(fast_key, (HEADS, STATE_ROW_COUNT), jnp.float32, jnp.log(0.04), jnp.log(0.12)))
    decay_rate = jnp.where(slow_head, slow_rate, fast_rate)
    return (1.0 - decay_rate).reshape(HEADS * STATE_ROW_COUNT).astype(jnp.float32)


def draw_extra_log_decay(key, part):
    location_seed, size_key = jax.random.split(key)
    spike_places = jax.random.randint(location_seed, (4,), 0, SEQUENCE_TOKENS)
    spike_mask = jnp.any(jnp.arange(SEQUENCE_TOKENS)[None, :] == spike_places[:, None], axis=0)
    retained_fraction = jax.random.uniform(size_key, (HEADS, 1), jnp.float32, 0.5, 0.8)
    return jnp.where(spike_mask[None, :], jnp.log(retained_fraction), 0.0).astype(jnp.float32)


def level_of(rng, dims, shards, least, largest):
    level = 1.0
    for dim, blocks in shards:
        heights = jax.random.uniform(jax.random.fold_in(jax.random.fold_in(rng, 6), dim), (blocks,), jnp.float32, least / len(shards), largest / len(shards))
        level = level * jnp.repeat(jnp.exp(heights), dims[dim] // blocks).reshape((-1,) + (1,) * (len(dims) - 1 - dim))
    return level


def assign_block(key, own, number, rows, number_of, top, reach, skew):
    ranking = jax.random.permutation(key, number_of)
    heavy_load, ordinary = portions_of(number_of, rows * top, reach, skew, True), portions_of(number_of, rows * top, reach, skew, False)
    places = jnp.arange(number_of)

    def named(tallies, rotation):
        used = int((tallies > 0).sum())
        fixed = max(1, used // 4)
        passed = fixed + (places - fixed + rotation * (used - fixed)) % max(1, number_of - fixed)
        return jnp.zeros((number_of,), jnp.int32).at[ranking[jnp.where(places < fixed, places, passed)]].set(jnp.asarray(tallies, jnp.int32))

    tallies = jnp.where(number % 4 == 0, named(heavy_load, number // 4), named(ordinary, number - number // 4 - 1))
    mixed = jax.random.permutation(jax.random.fold_in(own, 3), number_of)
    giver, taker = mixed[0:number_of // 2 * 2:2], mixed[1:number_of // 2 * 2:2]
    slack = jnp.minimum(tallies[giver] - 1, reach - tallies[taker]) // 2
    slack = jnp.where((giver == ranking[0]) | (taker == ranking[0]) | (tallies[taker] == 0), 0, jnp.maximum(slack, 0))
    passed = jax.random.randint(jax.random.fold_in(own, 4), (number_of // 2,), 0, 1 << 20) % (slack + 1)
    tallies = tallies.at[giver].add(-passed).at[taker].add(passed)
    members = jnp.searchsorted(jnp.cumsum(tallies), jnp.arange(rows * top), side="right").astype(jnp.int32)
    listing = members.reshape(top, rows).T
    listing = listing[jax.random.permutation(jax.random.fold_in(own, 1), rows)]
    rotation = jax.random.randint(jax.random.fold_in(own, 2), (rows, 1), 0, top)
    return jnp.take_along_axis(listing, (jnp.arange(top)[None, :] + rotation) % top, axis=1)


def portions_of(number_of, total, bound, lean, full):
    portions = [(1 << 20) // math.isqrt(standing ** lean) + 1 for standing in range(1, number_of + 1)]
    largest = bound if full else min(bound, max(-(-total // number_of), total * portions[0] // sum(portions)))
    least = 1 if total - largest >= number_of - 1 else 0
    holding, rest = [largest] + [least] * (number_of - 1), total - largest - least * (number_of - 1)
    while rest > 0:
        candidates = [i for i in range(1, number_of) if holding[i] < largest] or [i for i in range(1, number_of) if holding[i] < bound]
        pool, budget = sum([portions[i] for i in candidates]), rest
        for i in candidates:
            addition = min(bound - holding[i], max(1, budget * portions[i] // pool), rest)
            holding[i] = holding[i] + addition
            rest = rest - addition
    return np.array(holding)


def noise(rng, dims, scale, limit, pieces=(), kind=jnp.bfloat16):
    loudness = level_of(rng, dims, pieces, -0.22, 0.18) if pieces else 1.0
    values = jax.random.normal(rng, dims, jnp.float32) * scale * loudness
    return jnp.minimum(jnp.maximum(values, -limit), limit).astype(kind)


def setup_inputs(seed: int = 0) -> dict:
    streams_of = jax.random.split(jax.random.key(seed), 16)
    query = noise(streams_of[0], (SEQUENCE_TOKENS, KEY_WIDTH), 1.0, 6.0, ((0, 64), (1, 4)))
    forget_preact = draw_forget_preact(jax.random.fold_in(streams_of[15], 71), 0)
    value_input = noise(streams_of[2], (SEQUENCE_TOKENS, VALUE_WIDTH), 1.0, 6.0, ((0, 64), (1, 4)))
    output_gate = noise(streams_of[3], (SEQUENCE_TOKENS, VALUE_WIDTH), 1.0, 6.0, ((0, 64), (1, 4)))
    forget_minimum = draw_forget_minimum(jax.random.fold_in(streams_of[15], 71), 0)
    extra_log_decay = draw_extra_log_decay(jax.random.fold_in(streams_of[15], 71), 0)
    head_norm_gain = jnp.clip(1.0 + 0.18 * jax.random.normal(streams_of[6], (VALUE_WIDTH,), jnp.float32), 0.1, 1.9)
    output_weight = noise(streams_of[7], (VALUE_WIDTH, D), VALUE_WIDTH ** -0.5, 0.15625, ((1, 4),))
    stream = noise(streams_of[8], (SEQUENCE_TOKENS, D), 1.0, 6.0, ((0, 256),))
    feedforward_gain = jnp.clip(1.0 + 0.18 * jax.random.normal(streams_of[9], (D,), jnp.float32), 0.1, 1.9)
    routes_keys = jax.random.split(jax.random.fold_in(streams_of[10], 1), SEQUENCE_TOKENS // QROWS)
    routes_turns = jax.random.permutation(jax.random.fold_in(streams_of[10], 3), SEQUENCE_TOKENS // QROWS)
    routes = jax.vmap(lambda own, number: assign_block(jax.random.fold_in(streams_of[10], 2), own, number, QROWS, EXPERTS, TOPK, CAPQ, 2))(routes_keys, routes_turns).reshape((SEQUENCE_TOKENS, TOPK))
    router_weight = jnp.clip(0.05 + 0.95 * jax.random.uniform(streams_of[11], (SEQUENCE_TOKENS, TOPK), jnp.float32) ** level_of(streams_of[11], (SEQUENCE_TOKENS, TOPK), ((0, 256),), -0.2, 0.2), 0.05, 1.0)
    expert_gate_weight = noise(streams_of[12], (EXPERTS, D, FF), D ** -0.5, 0.109375, ((0, 64), (2, 4)))
    expert_up_weight = noise(streams_of[13], (EXPERTS, D, FF), D ** -0.5, 0.109375, ((0, 64), (2, 4)))
    expert_down_weight = noise(streams_of[14], (EXPERTS, FF, D), FF ** -0.5, 0.1875, ((0, 64), (1, 4)))
    return dict(query=query, forget_preact=forget_preact, value_input=value_input, output_gate=output_gate, forget_minimum=forget_minimum, extra_log_decay=extra_log_decay, head_norm_gain=head_norm_gain, output_weight=output_weight, stream=stream, feedforward_gain=feedforward_gain, routes=routes, router_weight=router_weight, expert_gate_weight=expert_gate_weight, expert_up_weight=expert_up_weight, expert_down_weight=expert_down_weight)


epsilon = 1e-06
top_precision = lax.Precision.HIGHEST
tile_rows = 256

def block_step(current_state, block_inputs):
    query_block, weight_blk, value_block, decay_blk = block_inputs
    running_decay = jnp.cumsum(decay_blk, axis=1)
    intermediate = jnp.einsum('yro,yow->yrw', query_block * jnp.exp(running_decay), current_state, precision=top_precision)
    causal = lax.broadcasted_iota(jnp.int32, (SPAN, SPAN), 0) >= lax.broadcasted_iota(jnp.int32, (SPAN, SPAN), 1)
    log_gap = running_decay[:, :, None, :] - running_decay[:, None, :, :]
    decay_table = jnp.exp(jnp.where(causal[None, :, :, None], log_gap, -jnp.inf))
    scores = jnp.einsum('htk,hsk,htsk->hts', query_block, weight_blk, decay_table, precision=top_precision)
    output = intermediate + jnp.einsum('hts,hsv->htv', scores, value_block, precision=top_precision)
    final_decay = running_decay[:, -1:, :]
    scaled_rows = weight_blk * jnp.exp(final_decay - running_decay)
    following_state = jnp.exp(final_decay[:, 0, :])[:, :, None] * current_state + jnp.einsum('xme,xmc->xec', scaled_rows, value_block, precision=top_precision)
    return (following_state, output)

def gate_factors(query, forget_preact, forget_minimum, extra_log_decay):
    query_activated = jax.nn.silu(query.astype(jnp.float32))
    incoming_weight = (1.0 - forget_minimum) * jax.nn.sigmoid(-forget_preact.astype(jnp.float32))
    spike_columns = jnp.repeat(jnp.transpose(extra_log_decay), STATE_ROW_COUNT, axis=1)
    decay_logarithm = jnp.log1p(-incoming_weight) + spike_columns
    return (query_activated, incoming_weight, decay_logarithm)

def head_blocks(array_in, head_total):
    rows_in = array_in.shape[0]
    return array_in.reshape(rows_in // SPAN, SPAN, head_total, -1).transpose(0, 2, 1, 3)

def head_output(mixed, head_norm_gain, output_gate):
    normalized = mixed * lax.rsqrt(lax.optimization_barrier(jnp.mean(mixed * mixed, axis=-1, keepdims=True)) + epsilon)
    flat_rows = normalized.reshape(mixed.shape[0], -1)
    return (flat_rows * head_norm_gain * jax.nn.silu(output_gate.astype(jnp.float32))).astype(jnp.bfloat16)

def rms_norm(residual, gain):
    scale_row = lax.rsqrt(lax.optimization_barrier(jnp.mean(residual * residual, axis=-1, keepdims=True)) + epsilon)
    return (residual * scale_row * gain).astype(jnp.bfloat16)

def expert_rows(row_data, gate_w, up_w, down_w):
    gate_act = jnp.dot(row_data, gate_w, preferred_element_type=jnp.float32)
    up_act = jnp.dot(row_data, up_w, preferred_element_type=jnp.float32)
    inner_act = (jax.nn.silu(gate_act) * up_act).astype(jnp.bfloat16)
    quarter = inner_act.shape[1] // N_TP
    parts = jnp.einsum('njf,jfd->njd', inner_act.reshape(-1, N_TP, quarter).astype(jnp.float32), down_w.reshape(N_TP, quarter, -1).astype(jnp.float32))
    parts = lax.optimization_barrier(parts.astype(jnp.bfloat16))
    return lax.optimization_barrier(jnp.sum(parts.astype(jnp.float32), axis=1)).astype(jnp.bfloat16)

def routed(normed, routes, route_weight, expert_gate_weight, expert_up_weight, expert_down_weight):
    pick_ids = routes.reshape(-1).astype(jnp.int32)
    flat_weight = route_weight.reshape(-1)
    expert_ids = jnp.arange(EXPERTS, dtype=jnp.int32)
    counts = lax.optimization_barrier(jnp.sum((pick_ids[:, None] == expert_ids[None, :]).astype(jnp.int32), axis=0)).astype(jnp.int32)
    starts = (jnp.cumsum(counts) - counts).astype(jnp.int32)
    sort_order = jnp.argsort(pick_ids, stable=True).astype(jnp.int32)
    padded = jnp.concatenate([sort_order, jnp.zeros((tile_rows,), jnp.int32)])
    result = jnp.zeros((normed.shape[0], normed.shape[1]), jnp.float32)

    def per_expert(expert_id, result_now):
        tile_count = ((counts[expert_id] + tile_rows - 1) // tile_rows).astype(jnp.int32)

        def per_tile(tile_id, result_tile):
            offset = (tile_id * tile_rows).astype(jnp.int32)
            row_ids = lax.dynamic_slice_in_dim(padded, (starts[expert_id] + offset).astype(jnp.int32), tile_rows)
            valid_rows = offset + jnp.arange(tile_rows, dtype=jnp.int32) < counts[expert_id]
            row_data = normed[row_ids // TOPK]
            output = expert_rows(row_data, expert_gate_weight[expert_id], expert_up_weight[expert_id], expert_down_weight[expert_id])
            weighted = jnp.where(valid_rows, flat_weight[row_ids], 0.0)[:, None] * output.astype(jnp.float32)
            return result_tile.at[row_ids // TOPK].add(weighted)
        return lax.fori_loop(jnp.int32(0), tile_count, per_tile, result_now)
    return lax.fori_loop(0, EXPERTS, per_expert, result)

def reference(query, forget_preact, value_input, output_gate, forget_minimum, extra_log_decay, head_norm_gain, output_weight, stream, feedforward_gain, routes, router_weight, expert_gate_weight, expert_up_weight, expert_down_weight):
    query_activated, incoming_weight, decay_logarithm = gate_factors(query, forget_preact, forget_minimum, extra_log_decay)
    value_rows = value_input.astype(jnp.float32)
    blocks = (head_blocks(query_activated, HEADS), head_blocks(incoming_weight, HEADS), head_blocks(value_rows, HEADS), head_blocks(decay_logarithm, HEADS))
    start_state = jnp.zeros((HEADS, STATE_ROW_COUNT, VALUE_CHANNELS), jnp.float32)
    _, block_outs = lax.scan(block_step, start_state, blocks)
    mixed = block_outs.transpose(0, 2, 1, 3).reshape(SEQUENCE_TOKENS, HEADS, VALUE_CHANNELS)
    hidden = head_output(mixed, head_norm_gain, output_gate)
    mix_rows = jnp.dot(hidden, output_weight, preferred_element_type=jnp.float32).astype(jnp.bfloat16)
    mix_rows = lax.optimization_barrier(mix_rows)
    residual = stream.astype(jnp.float32) + mix_rows.astype(jnp.float32)
    normed = rms_norm(residual, feedforward_gain)
    route_weight = router_weight / lax.optimization_barrier(jnp.sum(router_weight, axis=1, keepdims=True))
    routed_sum = routed(normed, routes, route_weight, expert_gate_weight, expert_up_weight, expert_down_weight)
    return (residual + routed_sum).astype(jnp.bfloat16)
```

```python
import jax
import jax.numpy as jnp
from jax import lax
from jax.experimental import pallas as pl
from jax.experimental.pallas import tpu as pltpu
from jax.sharding import Mesh
from jax.sharding import PartitionSpec as P

LANES = 128
SPAN = 64
TOPK = 2
PLANE = ("sp_1", "sp_2")
SP = ("sp_0", "sp_1", "sp_2")
TP = ("tp_0", "tp_1")
SP_TP = SP + TP
ROW_PAIRS = ((1, 2), (2, 1), (3, 0), (0, 3))

f32 = jnp.float32
bf16 = jnp.bfloat16
epsilon = 1e-06
exact = lax.Precision.HIGHEST


def dot(a, b, dims=((1,), (0,)), precision=None):
    return lax.dot_general(a, b, (dims, ((), ())), precision=precision, preferred_element_type=f32)


def split(value):
    high = value.astype(bf16)
    return high, (value - high.astype(f32)).astype(bf16)


def silu(value):
    return value * jax.nn.sigmoid(value)


def call(kernel, out_shape, *operands, smem=()):
    specs = [
        pl.BlockSpec(memory_space=pltpu.SMEM if k in smem else pltpu.VMEM)
        for k in range(len(operands))
    ]
    outs = jax.tree.map(lambda _: pl.BlockSpec(memory_space=pltpu.VMEM), out_shape)
    return pl.pallas_call(
        kernel,
        out_shape=out_shape,
        in_specs=specs,
        out_specs=outs,
        compiler_params=pltpu.CompilerParams(vmem_limit_bytes=48 * 1024 * 1024),
    )(*operands)


def decays(forget_ref, floor_ref, extra_ref, table):
    weight = (1.0 - floor_ref[...]) * jax.nn.sigmoid(-forget_ref[...].astype(f32))
    single = jnp.log1p(-weight)
    summed = dot(table, single, precision=exact)
    extra = extra_ref[...]
    extra_summed = dot(table, extra, ((1,), (1,)), precision=exact)
    return weight, summed, extra_summed


def state_kernel(forget_ref, value_ref, floor_ref, extra_ref, out_ref):
    rows, width = forget_ref.shape
    heads = width // LANES
    pieces = out_ref.shape[0]
    piece = LANES // pieces
    at = lax.broadcasted_iota(jnp.int32, (rows, rows), 0)
    other = lax.broadcasted_iota(jnp.int32, (rows, rows), 1)
    after = (other > at).astype(f32)
    weight, tail, extra_tail = decays(forget_ref, floor_ref, extra_ref, after)
    first = jnp.log1p(-weight[:1])
    row_at = lax.broadcasted_iota(jnp.int32, (16, LANES), 0)
    decay_rows = jnp.zeros((16, LANES), f32)
    for h in range(heads):
        lanes = slice(h * LANES, (h + 1) * LANES)
        rest = tail[:, lanes] + extra_tail[:, h : h + 1]
        total = rest[:1] + first[:, lanes] + extra_ref[h : h + 1, 0:1]
        high = total.astype(bf16).astype(f32)
        decay_rows = jnp.where(row_at == h, high, decay_rows)
        decay_rows = jnp.where(row_at == heads + h, total - high, decay_rows)
        scaled_high, scaled_low = split(weight[:, lanes] * jnp.exp(rest))
        value = value_ref[:, lanes]
        state = dot(value, scaled_high, ((0,), (0,))) + dot(value, scaled_low, ((0,), (0,)))
        for p in range(pieces):
            out_ref[p, h * piece : (h + 1) * piece, :] = state[p * piece : (p + 1) * piece].astype(bf16)
    for p in range(pieces):
        out_ref[p, heads * piece :, :] = decay_rows.astype(bf16)


def read_piece(ref, j, heads, piece):
    states = [ref[j, h * piece : (h + 1) * piece, :].astype(f32) for h in range(heads)]
    rows = ref[j, heads * piece :, :].astype(f32)
    totals = [rows[h : h + 1] + rows[heads + h : heads + h + 1] for h in range(heads)]
    return states, totals


def plane_kernel(heads, in_ref, out_ref, before_ref, passed_ref):
    members = in_ref.shape[0]
    piece = before_ref.shape[1] // heads
    running = [jnp.zeros((piece, LANES), f32) for _ in range(heads)]
    total = [jnp.zeros((1, LANES), f32) for _ in range(heads)]
    passed_ref[...] = jnp.zeros(passed_ref.shape, f32)
    for j in range(members):
        states, decay = read_piece(in_ref, j, heads, piece)
        for h in range(heads):
            before_ref[j, h * piece : (h + 1) * piece, :] = running[h]
            passed_ref[j, h : h + 1, :] = total[h]
            running[h] = jnp.exp(decay[h]) * running[h] + states[h]
            total[h] = total[h] + decay[h]
    row_at = lax.broadcasted_iota(jnp.int32, (16, LANES), 0)
    decay_rows = jnp.zeros((16, LANES), f32)
    for h in range(heads):
        high = total[h].astype(bf16).astype(f32)
        decay_rows = jnp.where(row_at == h, high, decay_rows)
        decay_rows = jnp.where(row_at == heads + h, total[h] - high, decay_rows)
    for k in range(out_ref.shape[0]):
        for h in range(heads):
            out_ref[k, h * piece : (h + 1) * piece, :] = running[h].astype(bf16)
        out_ref[k, heads * piece :, :] = decay_rows.astype(bf16)


def carry_kernel(heads, place_ref, in_ref, before_ref, passed_ref, out_ref):
    piece = before_ref.shape[1] // heads
    place = place_ref[0]
    running = [jnp.zeros((piece, LANES), f32) for _ in range(heads)]
    for k in range(in_ref.shape[0]):
        states, decay = read_piece(in_ref, k, heads, piece)
        for h in range(heads):
            following = jnp.exp(decay[h]) * running[h] + states[h]
            running[h] = jnp.where(k < place, following, running[h])
    for j in range(out_ref.shape[0]):
        for h in range(heads):
            rows = slice(h * piece, (h + 1) * piece)
            out_ref[j, rows, :] = (
                jnp.exp(passed_ref[j, h : h + 1, :]) * running[h] + before_ref[j, rows, :]
            ).astype(bf16)


def local_kernel(query_ref, forget_ref, value_ref, floor_ref, extra_ref, out_ref, late_ref):
    rows, width = query_ref.shape
    at = lax.broadcasted_iota(jnp.int32, (rows, rows), 0)
    other = lax.broadcasted_iota(jnp.int32, (rows, rows), 1)
    upto = ((other <= at) & (at // SPAN == other // SPAN)).astype(f32)
    weight, summed, extra_summed = decays(forget_ref, floor_ref, extra_ref, upto)
    query = silu(query_ref[...].astype(f32))
    causal = lax.broadcasted_iota(jnp.int32, (SPAN, SPAN), 0) >= lax.broadcasted_iota(
        jnp.int32, (SPAN, SPAN), 1
    )
    for h in range(width // LANES):
        lanes = slice(h * LANES, (h + 1) * LANES)
        running = summed[:, lanes] + extra_summed[:, h : h + 1]
        asked = query[:, lanes] * jnp.exp(running)
        state = jnp.zeros((LANES, LANES), f32)
        passed = jnp.zeros((1, LANES), f32)
        for b in range(rows // SPAN):
            part = slice(b * SPAN, (b + 1) * SPAN)
            decay = running[part]
            final = decay[SPAN - 1 :]
            asked_now = asked[part].astype(bf16)
            value = value_ref[part, lanes]
            given = weight[part, lanes]
            scores = dot(asked_now, (given * jnp.exp(-decay)).astype(bf16), ((1,), (1,)))
            scores = jnp.where(causal, scores, 0.0).astype(bf16)
            out = dot(scores, value)
            if b:
                out = out + dot(asked_now, state.astype(bf16), ((1,), (1,)))
            out_ref[part, lanes] = out
            late_ref[part, lanes] = (asked[part] * jnp.exp(passed)).astype(bf16)
            passed = passed + final
            kept = (given * jnp.exp(final - decay)).astype(bf16)
            state = state * jnp.exp(final) + dot(value, kept, ((0,), (0,)))


def head_kernel(local_ref, late_ref, carry_ref, gain_ref, gate_ref, out_ref):
    width = local_ref.shape[1]
    heads = width // LANES
    piece = carry_ref.shape[1] // heads
    for h in range(heads):
        lanes = slice(h * LANES, (h + 1) * LANES)
        carried = jnp.concatenate(
            [carry_ref[p, h * piece : (h + 1) * piece, :] for p in range(carry_ref.shape[0])], axis=0
        )
        mixed = local_ref[:, lanes] + dot(late_ref[:, lanes], carried, ((1,), (1,)))
        scale = lax.rsqrt(jnp.mean(mixed * mixed, axis=-1, keepdims=True) + epsilon)
        gate = silu(gate_ref[:, lanes].astype(f32))
        hidden = (mixed * scale * gain_ref[:, lanes] * gate).astype(bf16)
        for k in range(out_ref.shape[0]):
            out_ref[k, :, lanes] = hidden


def slots_in_row(column_ref, row_ref, capacity):
    tokens = column_ref.shape[0]
    earlier = lax.broadcasted_iota(jnp.int32, (tokens, tokens), 0) < lax.broadcasted_iota(
        jnp.int32, (tokens, tokens), 1
    )
    slots = []
    for j in range(TOPK):
        mine = row_ref[j : j + 1, :]
        rank = jnp.zeros((1, tokens), f32)
        for i in range(j + 1):
            same = column_ref[:, i : i + 1] == mine
            if i == j:
                same = same & earlier
            rank = rank + jnp.sum(same.astype(f32), axis=0, keepdims=True)
        slots.append(mine * capacity + rank.astype(jnp.int32))
    return slots


def slots_in_column(column_ref, row_ref, capacity):
    tokens = column_ref.shape[0]
    earlier = lax.broadcasted_iota(jnp.int32, (tokens, tokens), 1) < lax.broadcasted_iota(
        jnp.int32, (tokens, tokens), 0
    )
    slots = []
    for j in range(TOPK):
        mine = column_ref[:, j : j + 1]
        rank = jnp.zeros((tokens, 1), f32)
        for i in range(j + 1):
            same = row_ref[i : i + 1, :] == mine
            if i == j:
                same = same & earlier
            rank = rank + jnp.sum(same.astype(f32), axis=1, keepdims=True)
        slots.append(mine * capacity + rank.astype(jnp.int32))
    return slots


def dispatch_kernel(capacity, mix_ref, stream_ref, gain_ref, column_ref, row_ref, residual_ref, *send_refs):
    tokens, width = stream_ref.shape
    blocks, _, block = mix_ref.shape
    square = jnp.zeros((tokens, 1), f32)
    for k in range(blocks):
        lanes = slice(k * block, (k + 1) * block)
        residual = stream_ref[:, lanes].astype(f32) + mix_ref[k].astype(f32)
        residual_ref[:, lanes] = residual
        square = square + jnp.sum(residual * residual, axis=1, keepdims=True)
    scale = lax.rsqrt(square / width + epsilon)
    slots = slots_in_row(column_ref, row_ref, capacity)
    slot_at = lax.broadcasted_iota(jnp.int32, (send_refs[0].shape[0], tokens), 0)
    table = ((slot_at == slots[0]) | (slot_at == slots[1])).astype(f32).astype(bf16)
    part = width // len(send_refs)
    for k, send_ref in enumerate(send_refs):
        lanes = slice(k * part, (k + 1) * part)
        normed = (residual_ref[:, lanes] * scale * gain_ref[:, lanes]).astype(bf16)
        send_ref[...] = dot(table, normed).astype(bf16)


def combine_kernel(capacity, results_ref, residual_ref, column_ref, row_ref, weight_ref, out_ref):
    tokens = residual_ref.shape[0]
    slots = slots_in_column(column_ref, row_ref, capacity)
    weight = weight_ref[...]
    weight = weight / jnp.sum(weight, axis=1, keepdims=True)
    slot_at = lax.broadcasted_iota(jnp.int32, (tokens, results_ref.shape[0]), 1)
    table = jnp.zeros((tokens, results_ref.shape[0]), f32)
    for j in range(TOPK):
        table = table + jnp.where(slot_at == slots[j], weight[:, j : j + 1], 0.0)
    high, low = split(table)
    results = results_ref[...]
    out_ref[...] = (residual_ref[...] + (dot(high, results) + dot(low, results))).astype(bf16)


def spread(value, axes):
    return lax.all_to_all(value, axes, split_axis=0, concat_axis=0, tiled=True)


def per_device(
    query,
    forget_preact,
    value_input,
    output_gate,
    forget_minimum,
    extra_log_decay,
    head_norm_gain,
    output_weight,
    stream,
    feedforward_gain,
    routes,
    router_weight,
    expert_gate_weight,
    expert_up_weight,
    expert_down_weight,
):
    window_rows, width = query.shape
    heads = width // LANES
    tp_size = lax.axis_size(TP)
    sp_size = lax.axis_size(SP)
    plane = lax.axis_size(PLANE)
    planes = lax.axis_size("sp_0")
    quarter_rows, model_width = stream.shape
    capacity = window_rows // sp_size
    piece = LANES // plane

    both = jnp.stack([expert_gate_weight[0], expert_up_weight[0]])
    paired = lax.all_gather(both, "tp_1")
    down = lax.all_gather(expert_down_weight[0], TP)

    floor = forget_minimum.reshape(1, -1)
    message = jax.ShapeDtypeStruct((plane, heads * piece + 16, LANES), bf16)
    states = call(state_kernel, message, forget_preact, value_input, floor, extra_log_decay)
    states = spread(states, PLANE)
    totals, before, passed = call(
        lambda *refs: plane_kernel(heads, *refs),
        (
            jax.ShapeDtypeStruct((planes, heads * piece + 16, LANES), bf16),
            jax.ShapeDtypeStruct((plane, heads * piece, LANES), f32),
            jax.ShapeDtypeStruct((plane, 8, LANES), f32),
        ),
        states,
    )
    totals = spread(totals, "sp_0")
    local, late = call(
        local_kernel,
        (
            jax.ShapeDtypeStruct((window_rows, width), f32),
            jax.ShapeDtypeStruct((window_rows, width), bf16),
        ),
        query,
        forget_preact,
        value_input,
        floor,
        extra_log_decay,
    )
    place = lax.axis_index("sp_0").astype(jnp.int32).reshape(1)
    carried = call(
        lambda *refs: carry_kernel(heads, *refs),
        jax.ShapeDtypeStruct((plane, heads * piece, LANES), bf16),
        place,
        totals,
        before,
        passed,
        smem=(0,),
    )
    carried = spread(carried, PLANE)
    hidden = call(
        head_kernel,
        jax.ShapeDtypeStruct((tp_size, window_rows, width), bf16),
        local,
        late,
        carried,
        head_norm_gain.reshape(1, -1),
        output_gate,
    )
    hidden = spread(hidden, TP)
    projected = jnp.einsum(
        "ptc,pcd->td",
        hidden,
        output_weight.reshape(tp_size, width, -1),
        preferred_element_type=f32,
    ).astype(bf16)
    mix = spread(projected.reshape(tp_size, quarter_rows, -1), TP)

    own = lax.dynamic_slice_in_dim(routes, lax.axis_index(TP) * quarter_rows, quarter_rows, 0)
    own_rows = own.T
    halves = 2
    half = model_width // halves
    residual, *sends = call(
        lambda *refs: dispatch_kernel(capacity, *refs),
        (jax.ShapeDtypeStruct((quarter_rows, model_width), f32),)
        + (jax.ShapeDtypeStruct((window_rows, half), bf16),) * halves,
        mix,
        stream,
        feedforward_gain.reshape(1, -1),
        own,
        own_rows,
    )
    hidden_part = expert_gate_weight.shape[2]
    acts = 0.0
    for k, send in enumerate(sends):
        received = spread(send.reshape(sp_size, capacity, half), SP).reshape(window_rows, half)
        others = lax.ppermute(received, TP, ROW_PAIRS)
        rows = jnp.stack([received, others])
        weights = lax.slice_in_dim(paired, k * half, (k + 1) * half, axis=2)
        acts = acts + jnp.einsum("std,pgdf->gstpf", rows, weights, preferred_element_type=f32)
    inner = (silu(acts[0]) * acts[1]).astype(bf16)
    mine, theirs = inner[0], inner[1]
    rest = lax.ppermute(theirs, TP, ROW_PAIRS)
    first_half = lax.axis_index("tp_0") == 0
    inner = jnp.concatenate(
        [jnp.where(first_half, mine, rest), jnp.where(first_half, rest, mine)], axis=1
    ).reshape(window_rows, tp_size * hidden_part)
    expert_out = jnp.dot(
        inner, down.reshape(tp_size * hidden_part, model_width), preferred_element_type=f32
    ).astype(bf16)
    returned = spread(expert_out.reshape(sp_size, capacity, model_width), SP)
    return call(
        lambda *refs: combine_kernel(capacity, *refs),
        jax.ShapeDtypeStruct((quarter_rows, model_width), bf16),
        returned.reshape(window_rows, model_width),
        residual,
        own,
        own_rows,
        router_weight,
    )


def solution(mesh):
    torus = Mesh(mesh.devices.reshape(8, 4, 2, 2, 2), SP_TP)
    placed = (
        P(SP, TP),
        P(SP, TP),
        P(SP, TP),
        P(SP, TP),
        P(TP),
        P(TP, SP),
        P(TP),
        P(None, TP),
        P(SP_TP, None),
        P(),
        P(SP, None),
        P(SP_TP, None),
        P(SP, None, TP),
        P(SP, None, TP),
        P(SP, TP, None),
    )
    return jax.shard_map(
        per_device, mesh=torus, in_specs=placed, out_specs=P(SP_TP, None), check_vma=False
    )
```

```python
import jax
import jax.numpy as jnp
from jax import lax
from jax.experimental import pallas as pl
from jax.experimental.pallas import tpu as pltpu
from jax.sharding import Mesh
from jax.sharding import PartitionSpec as P


LANES = 128
SPAN = 64
PARTS = 2
DOWN_LANES = 512
TOPK = 2
PLANE = ("sp_1", "sp_2")
SP = ("sp_0", "sp_1", "sp_2")
TP = ("tp_0", "tp_1")
SP_TP = SP + TP
ROW_PAIRS = ((1, 2), (2, 1), (3, 0), (0, 3))
WEIGHT_PAIRS = ((0, 1), (1, 0), (2, 3), (3, 2))
FIRST_SHARE = (2, 3)

f32 = jnp.float32
bf16 = jnp.bfloat16
epsilon = 1e-06
exact = lax.Precision.HIGHEST


def dot(a, b, dims=((1,), (0,)), precision=None):
    return lax.dot_general(a, b, (dims, ((), ())), precision=precision, preferred_element_type=f32)


def split(value):
    high = value.astype(bf16)
    return high, (value - high.astype(f32)).astype(bf16)


def silu(value):
    return value * jax.nn.sigmoid(value)


def call(kernel, out_shape, *operands, kinds="", scratch=(), mib=12):
    spaces = {
        "v": pl.BlockSpec(memory_space=pltpu.VMEM),
        "h": pl.BlockSpec(memory_space=pltpu.HBM),
        "s": pl.BlockSpec(memory_space=pltpu.SMEM),
    }
    kinds = kinds or "v" * len(operands)
    return pl.pallas_call(
        kernel,
        out_shape=out_shape,
        in_specs=[spaces[kind] for _, kind in zip(operands, kinds, strict=True)],
        out_specs=jax.tree.map(lambda _: spaces["v"], out_shape),
        scratch_shapes=scratch,
        compiler_params=pltpu.CompilerParams(vmem_limit_bytes=mib * 1024 * 1024),
    )(*operands)


def decays(forget_ref, floor_ref, extra_ref, table):
    weight = (1.0 - floor_ref[...]) * jax.nn.sigmoid(-forget_ref[...].astype(f32))
    single = jnp.log1p(-weight)
    summed = dot(table, single, precision=exact)
    extra = extra_ref[...]
    extra_summed = dot(table, extra, ((1,), (1,)), precision=exact)
    return weight, summed, extra_summed


def state_kernel(forget_ref, value_ref, floor_ref, extra_ref, out_ref):
    rows, width = forget_ref.shape
    heads = width // LANES
    pieces = out_ref.shape[0]
    piece = LANES // pieces
    at = lax.broadcasted_iota(jnp.int32, (rows, rows), 0)
    other = lax.broadcasted_iota(jnp.int32, (rows, rows), 1)
    after = (other > at).astype(f32)
    weight, tail, extra_tail = decays(forget_ref, floor_ref, extra_ref, after)
    first = jnp.log1p(-weight[:1])
    row_at = lax.broadcasted_iota(jnp.int32, (16, LANES), 0)
    decay_rows = jnp.zeros((16, LANES), f32)
    for h in range(heads):
        lanes = slice(h * LANES, (h + 1) * LANES)
        rest = tail[:, lanes] + extra_tail[:, h : h + 1]
        total = rest[:1] + first[:, lanes] + extra_ref[h : h + 1, 0:1]
        high = total.astype(bf16).astype(f32)
        decay_rows = jnp.where(row_at == h, high, decay_rows)
        decay_rows = jnp.where(row_at == heads + h, total - high, decay_rows)
        scaled_high, scaled_low = split(weight[:, lanes] * jnp.exp(rest))
        value = value_ref[:, lanes]
        state = dot(value, scaled_high, ((0,), (0,))) + dot(value, scaled_low, ((0,), (0,)))
        for p in range(pieces):
            out_ref[p, h * piece : (h + 1) * piece, :] = state[p * piece : (p + 1) * piece].astype(bf16)
    for p in range(pieces):
        out_ref[p, heads * piece :, :] = decay_rows.astype(bf16)


def read_piece(ref, j, heads, piece):
    states = [ref[j, h * piece : (h + 1) * piece, :].astype(f32) for h in range(heads)]
    rows = ref[j, heads * piece :, :].astype(f32)
    totals = [rows[h : h + 1] + rows[heads + h : heads + h + 1] for h in range(heads)]
    return states, totals


def plane_kernel(heads, in_ref, out_ref, before_ref, passed_ref):
    members = in_ref.shape[0]
    piece = before_ref.shape[1] // heads
    running = [jnp.zeros((piece, LANES), f32) for _ in range(heads)]
    total = [jnp.zeros((1, LANES), f32) for _ in range(heads)]
    passed_ref[...] = jnp.zeros(passed_ref.shape, f32)
    for j in range(members):
        states, decay = read_piece(in_ref, j, heads, piece)
        for h in range(heads):
            before_ref[j, h * piece : (h + 1) * piece, :] = running[h]
            passed_ref[j, h : h + 1, :] = total[h]
            running[h] = jnp.exp(decay[h]) * running[h] + states[h]
            total[h] = total[h] + decay[h]
    row_at = lax.broadcasted_iota(jnp.int32, (16, LANES), 0)
    decay_rows = jnp.zeros((16, LANES), f32)
    for h in range(heads):
        high = total[h].astype(bf16).astype(f32)
        decay_rows = jnp.where(row_at == h, high, decay_rows)
        decay_rows = jnp.where(row_at == heads + h, total[h] - high, decay_rows)
    for k in range(out_ref.shape[0]):
        for h in range(heads):
            out_ref[k, h * piece : (h + 1) * piece, :] = running[h].astype(bf16)
        out_ref[k, heads * piece :, :] = decay_rows.astype(bf16)


def carry_kernel(heads, place_ref, in_ref, before_ref, passed_ref, out_ref):
    piece = before_ref.shape[1] // heads
    place = place_ref[0]
    running = [jnp.zeros((piece, LANES), f32) for _ in range(heads)]
    for k in range(in_ref.shape[0]):
        states, decay = read_piece(in_ref, k, heads, piece)
        for h in range(heads):
            following = jnp.exp(decay[h]) * running[h] + states[h]
            running[h] = jnp.where(k < place, following, running[h])
    for j in range(out_ref.shape[0]):
        for h in range(heads):
            rows = slice(h * piece, (h + 1) * piece)
            out_ref[j, rows, :] = (
                jnp.exp(passed_ref[j, h : h + 1, :]) * running[h] + before_ref[j, rows, :]
            ).astype(bf16)


def local_kernel(query_ref, forget_ref, value_ref, floor_ref, extra_ref, out_ref):
    rows, width = query_ref.shape
    at = lax.broadcasted_iota(jnp.int32, (rows, rows), 0)
    other = lax.broadcasted_iota(jnp.int32, (rows, rows), 1)
    upto = ((other <= at) & (at // SPAN == other // SPAN)).astype(f32)
    weight, summed, extra_summed = decays(forget_ref, floor_ref, extra_ref, upto)
    query = silu(query_ref[...].astype(f32))
    causal = lax.broadcasted_iota(jnp.int32, (SPAN, SPAN), 0) >= lax.broadcasted_iota(
        jnp.int32, (SPAN, SPAN), 1
    )
    for h in range(width // LANES):
        lanes = slice(h * LANES, (h + 1) * LANES)
        running = summed[:, lanes] + extra_summed[:, h : h + 1]
        asked = query[:, lanes] * jnp.exp(running)
        state = jnp.zeros((LANES, LANES), f32)
        passed = jnp.zeros((1, LANES), f32)
        for b in range(rows // SPAN):
            part = slice(b * SPAN, (b + 1) * SPAN)
            decay = running[part]
            final = decay[SPAN - 1 :]
            asked_now = asked[part].astype(bf16)
            value = value_ref[part, lanes]
            given = weight[part, lanes]
            scores = dot(asked_now, (given * jnp.exp(-decay)).astype(bf16), ((1,), (1,)))
            scores = jnp.where(causal, scores, 0.0).astype(bf16)
            out = dot(scores, value)
            if b:
                out = out + dot(asked_now, state.astype(bf16), ((1,), (1,)))
            out_ref[0, part, lanes] = out
            out_ref[1, part, lanes] = asked[part] * jnp.exp(passed)
            passed = passed + final
            kept = (given * jnp.exp(final - decay)).astype(bf16)
            state = state * jnp.exp(final) + dot(value, kept, ((0,), (0,)))


def head_kernel(local_ref, carry_ref, gain_ref, gate_ref, out_ref):
    width = local_ref.shape[2]
    heads = width // LANES
    piece = carry_ref.shape[1] // heads
    for h in range(heads):
        lanes = slice(h * LANES, (h + 1) * LANES)
        carried = jnp.concatenate(
            [carry_ref[p, h * piece : (h + 1) * piece, :] for p in range(carry_ref.shape[0])], axis=0
        )
        late = local_ref[1, :, lanes].astype(bf16)
        mixed = local_ref[0, :, lanes] + dot(late, carried, ((1,), (1,)))
        scale = lax.rsqrt(jnp.mean(mixed * mixed, axis=-1, keepdims=True) + epsilon)
        gate = silu(gate_ref[:, lanes].astype(f32))
        hidden = (mixed * scale * gain_ref[:, lanes] * gate).astype(bf16)
        for k in range(out_ref.shape[0]):
            out_ref[k, :, lanes] = hidden


def slots_in_row(column_ref, row_ref, capacity):
    tokens = column_ref.shape[0]
    earlier = lax.broadcasted_iota(jnp.int32, (tokens, tokens), 0) < lax.broadcasted_iota(
        jnp.int32, (tokens, tokens), 1
    )
    slots = []
    for j in range(TOPK):
        mine = row_ref[j : j + 1, :]
        rank = jnp.zeros((1, tokens), f32)
        for i in range(j + 1):
            same = column_ref[:, i : i + 1] == mine
            if i == j:
                same = same & earlier
            rank = rank + jnp.sum(same.astype(f32), axis=0, keepdims=True)
        slots.append(mine * (PARTS * capacity) + rank.astype(jnp.int32))
    return slots


def slots_in_column(column_ref, row_ref, capacity):
    tokens = column_ref.shape[0]
    earlier = lax.broadcasted_iota(jnp.int32, (tokens, tokens), 1) < lax.broadcasted_iota(
        jnp.int32, (tokens, tokens), 0
    )
    slots = []
    for j in range(TOPK):
        mine = column_ref[:, j : j + 1]
        rank = jnp.zeros((tokens, 1), f32)
        for i in range(j + 1):
            same = row_ref[i : i + 1, :] == mine
            if i == j:
                same = same & earlier
            rank = rank + jnp.sum(same.astype(f32), axis=1, keepdims=True)
        slots.append(mine * (PARTS * capacity) + rank.astype(jnp.int32))
    return slots


def spread_table(rows, columns, capacity, part):
    row = lax.broadcasted_iota(jnp.int32, (rows, columns), 0)
    column = lax.broadcasted_iota(jnp.int32, (rows, columns), 1)
    stride = PARTS * capacity
    wanted = (column // capacity) * stride + part * capacity + column % capacity
    return (row == wanted).astype(f32).astype(bf16)


def gather_table(rows, columns, capacity, part):
    row = lax.broadcasted_iota(jnp.int32, (rows, columns), 0)
    column = lax.broadcasted_iota(jnp.int32, (rows, columns), 1)
    stride = PARTS * capacity
    wanted = (row // capacity) * stride + part * capacity + row % capacity
    return (column == wanted).astype(f32).astype(bf16)


def dispatch_kernel(capacity, mix_ref, stream_ref, gain_ref, column_ref, row_ref, residual_ref, *send_refs):
    tokens, width = stream_ref.shape
    blocks, _, block = mix_ref.shape
    square = jnp.zeros((tokens, 1), f32)
    for k in range(blocks):
        lanes = slice(k * block, (k + 1) * block)
        residual = stream_ref[:, lanes].astype(f32) + mix_ref[k].astype(f32)
        residual_ref[:, lanes] = residual
        square = square + jnp.sum(residual * residual, axis=1, keepdims=True)
    scale = lax.rsqrt(square / width + epsilon)
    slots = slots_in_row(column_ref, row_ref, capacity)
    slot_at = lax.broadcasted_iota(jnp.int32, (send_refs[0].shape[0], tokens), 0)
    tables = [
        ((slot_at == slots[0] + q * capacity) | (slot_at == slots[1] + q * capacity))
        .astype(f32)
        .astype(bf16)
        for q in range(PARTS)
    ]
    start = 0
    for send_ref in send_refs:
        part = send_ref.shape[1]
        send = jnp.zeros(send_ref.shape, f32)
        for q in range(PARTS):
            lanes = slice(start, start + part)
            start += part
            normed = (residual_ref[:, lanes] * scale * gain_ref[:, lanes]).astype(bf16)
            send = send + dot(tables[q], normed)
        send_ref[...] = send.astype(bf16)


def gate_up(own_ref, others_ref, weight_refs, capacity):
    rows, part = own_ref.shape
    tables = [gather_table(rows // PARTS, rows, capacity, q) for q in range(PARTS)]
    laid = [
        jnp.concatenate([dot(table, ref[...]).astype(bf16) for table in tables], axis=1)
        for ref in (own_ref, others_ref)
    ]
    for j, weight_ref in enumerate(weight_refs):
        weight = weight_ref[: PARTS * part, :]
        for i in range(2):
            yield i, j, dot(laid[i], weight)


def first_kernel(
    capacity, own_ref, others_ref, gate_ref, gate_too_ref, up_pair_ref, parts_ref, acts_ref, kept_ref
):
    place = parts_ref[0] % 2
    weight_refs = (gate_ref, up_pair_ref.at[place], gate_too_ref, up_pair_ref.at[1 - place])
    for i, j, product in gate_up(own_ref, others_ref, weight_refs, capacity):
        acts_ref[i, j] = product
    left = kept_ref.shape[1]
    for j, weight_ref in enumerate(weight_refs):
        kept_ref[j] = weight_ref[weight_ref.shape[0] - left :, :]


def second_kernel(capacity, own_ref, others_ref, kept_ref, acts_ref, mine_ref, theirs_ref):
    outs = (mine_ref, theirs_ref)
    width = kept_ref.shape[2]
    gates = {}
    weight_refs = [kept_ref.at[j] for j in range(kept_ref.shape[0])]
    for i, j, product in gate_up(own_ref, others_ref, weight_refs, capacity):
        product = product + acts_ref[i, j]
        if j % 2 == 0:
            gates[i] = silu(product)
        else:
            lanes = slice(j // 2 * width, (j // 2 + 1) * width)
            outs[i][:, lanes] = (gates[i] * product).astype(bf16)


def down_kernel(capacity, parts_ref, mine_ref, rest_ref, weights_ref, out_ref):
    width = weights_ref.shape[1]
    inner = [ref[:, k * width : (k + 1) * width] for ref in (mine_ref, rest_ref) for k in range(2)]
    rows = mine_ref.shape[0]
    block = out_ref.shape[1]
    part = weights_ref.shape[2] // PARTS
    out = jnp.zeros(out_ref.shape, f32)
    for q in range(PARTS):
        lanes = pl.ds(pl.multiple_of(q * part + pl.program_id(0) * block, LANES), block)
        product = dot(inner[0], weights_ref[parts_ref[0], :, lanes])
        for k in range(1, len(inner)):
            product = product + dot(inner[k], weights_ref[parts_ref[k], :, lanes])
        out = out + dot(spread_table(PARTS * rows, rows, capacity, q), product.astype(bf16))
    out_ref[...] = out.astype(bf16)


def project_down(capacity, parts, mine, rest, weights):
    rows = mine.shape[0]
    part = weights.shape[2] // PARTS
    whole = pl.BlockSpec(memory_space=pltpu.VMEM)
    return pl.pallas_call(
        lambda *refs: down_kernel(capacity, *refs),
        grid=(part // DOWN_LANES,),
        out_shape=jax.ShapeDtypeStruct((PARTS * rows, part), bf16),
        in_specs=[pl.BlockSpec(memory_space=pltpu.SMEM), whole, whole, whole],
        out_specs=pl.BlockSpec((PARTS * rows, DOWN_LANES), lambda k: (0, k)),
        compiler_params=pltpu.CompilerParams(vmem_limit_bytes=12 * 1024 * 1024),
    )(parts, mine, rest, weights)


def combine_kernel(capacity, results_ref, residual_ref, column_ref, row_ref, weight_ref, out_ref):
    tokens = residual_ref.shape[0]
    slots = slots_in_column(column_ref, row_ref, capacity)
    weight = weight_ref[...]
    weight = weight / jnp.sum(weight, axis=1, keepdims=True)
    count, part = results_ref.shape
    for q in range(PARTS):
        slot_at = lax.broadcasted_iota(jnp.int32, (tokens, count), 1) - q * capacity
        table = jnp.zeros((tokens, count), f32)
        for j in range(TOPK):
            table = table + jnp.where(slot_at == slots[j], weight[:, j : j + 1], 0.0)
        high, low = split(table)
        results = results_ref[...]
        lanes = slice(q * part, (q + 1) * part)
        routed = dot(high, results) + dot(low, results)
        out_ref[:, lanes] = (residual_ref[:, lanes] + routed).astype(bf16)


def spread(value, axes):
    return lax.all_to_all(value, axes, split_axis=0, concat_axis=0, tiled=True)


def layer(
    query,
    forget_preact,
    value_input,
    output_gate,
    forget_minimum,
    extra_log_decay,
    head_norm_gain,
    output_weight,
    stream,
    feedforward_gain,
    routes,
    router_weight,
    expert_gate_weight,
    expert_up_weight,
    expert_down_weight,
):
    window_rows, width = query.shape
    heads = width // LANES
    tp_size = lax.axis_size(TP)
    sp_size = lax.axis_size(SP)
    plane = lax.axis_size(PLANE)
    planes = lax.axis_size("sp_0")
    quarter_rows, model_width = stream.shape
    capacity = window_rows // sp_size
    piece = LANES // plane

    down = lax.all_gather(expert_down_weight[0], TP)

    up_pair = lax.all_gather(expert_up_weight[0], "tp_1")

    floor = forget_minimum.reshape(1, -1)
    message = jax.ShapeDtypeStruct((plane, heads * piece + 16, LANES), bf16)
    states = call(
        state_kernel, message, forget_preact, value_input, floor, extra_log_decay
    )
    states = spread(states, PLANE)
    totals, before, passed = call(
        lambda *refs: plane_kernel(heads, *refs),
        (
            jax.ShapeDtypeStruct((planes, heads * piece + 16, LANES), bf16),
            jax.ShapeDtypeStruct((plane, heads * piece, LANES), f32),
            jax.ShapeDtypeStruct((plane, 8, LANES), f32),
        ),
        states,
    )
    totals = spread(totals, "sp_0")
    local = call(
        local_kernel,
        jax.ShapeDtypeStruct((2, window_rows, width), f32),
        query,
        forget_preact,
        value_input,
        floor,
        extra_log_decay,
    )
    place = lax.axis_index("sp_0").astype(jnp.int32).reshape(1)
    carried = call(
        lambda *refs: carry_kernel(heads, *refs),
        jax.ShapeDtypeStruct((plane, heads * piece, LANES), bf16),
        place,
        totals,
        before,
        passed,
        kinds="svvv",
    )
    carried = spread(carried, PLANE)
    hidden = call(
        head_kernel,
        jax.ShapeDtypeStruct((tp_size, window_rows, width), bf16),
        local,
        carried,
        head_norm_gain.reshape(1, -1),
        output_gate,
    )
    hidden = spread(hidden, TP)
    projected = jnp.einsum(
        "ptc,pcd->td",
        hidden,
        output_weight.reshape(tp_size, width, -1),
        preferred_element_type=f32,
    ).astype(bf16)
    mix = spread(projected.reshape(tp_size, quarter_rows, -1), TP)
    gate_weight, mix = lax.optimization_barrier((expert_gate_weight[0], mix))
    gate_weight_too = lax.ppermute(gate_weight, TP, WEIGHT_PAIRS)

    own = lax.dynamic_slice_in_dim(routes, lax.axis_index(TP) * quarter_rows, quarter_rows, 0)
    own_rows = own.T
    first_depth = model_width * FIRST_SHARE[0] // FIRST_SHARE[1]
    packed = [
        jax.ShapeDtypeStruct((window_rows * PARTS, depth // PARTS), bf16)
        for depth in (first_depth, model_width - first_depth)
    ]
    residual, *sends = call(
        lambda *refs: dispatch_kernel(capacity, *refs),
        (jax.ShapeDtypeStruct((quarter_rows, model_width), f32), *packed),
        mix,
        stream,
        feedforward_gain.reshape(1, -1),
        own,
        own_rows,
    )
    hidden_part = expert_gate_weight.shape[2]
    rows = []
    for send in sends:
        received = spread(send.reshape(sp_size, PARTS * capacity, -1), SP).reshape(send.shape)
        rows.append((received, lax.ppermute(received, TP, ROW_PAIRS)))
    count = 4
    place = lax.axis_index(TP).astype(jnp.int32)
    parts = jnp.stack([place, place ^ 1, 3 - place, (3 - place) ^ 1])
    acts, kept = call(
        lambda *refs: first_kernel(capacity, *refs),
        (
            jax.ShapeDtypeStruct((2, count, window_rows, hidden_part), f32),
            jax.ShapeDtypeStruct((count, model_width - first_depth, hidden_part), bf16),
        ),
        *rows[0],
        gate_weight,
        gate_weight_too,
        up_pair,
        parts,
        kinds="vvvvvs",
        mib=16,
    )
    acts, down = lax.optimization_barrier((acts, down))
    mine, theirs = call(
        lambda *refs: second_kernel(capacity, *refs),
        (jax.ShapeDtypeStruct((window_rows, 2 * hidden_part), bf16),) * 2,
        *rows[1],
        kept,
        acts,
    )
    rest = lax.ppermute(theirs, TP, ROW_PAIRS)
    expert_out = project_down(
        capacity,
        parts,
        mine,
        rest,
        down,
    )
    returned = spread(expert_out.reshape(sp_size, PARTS * capacity, -1), SP)
    return call(
        lambda *refs: combine_kernel(capacity, *refs),
        jax.ShapeDtypeStruct((quarter_rows, model_width), bf16),
        returned.reshape(expert_out.shape),
        residual,
        own,
        own_rows,
        router_weight,
    )


def solution(mesh):
    torus = Mesh(mesh.devices.reshape(8, 4, 2, 2, 2), SP_TP)
    placed = (
        P(SP, TP),
        P(SP, TP),
        P(SP, TP),
        P(SP, TP),
        P(TP),
        P(TP, SP),
        P(TP),
        P(None, TP),
        P(SP_TP, None),
        P(),
        P(SP, None),
        P(SP_TP, None),
        P(SP, None, TP),
        P(SP, None, TP),
        P(SP, TP, None),
    )
    return jax.shard_map(
        layer, mesh=torus, in_specs=placed, out_specs=P(SP_TP, None), check_vma=False
    )
```

```python
import jax
import jax.numpy as jnp
from jax import lax
from jax.experimental import pallas as pl
from jax.experimental.pallas import tpu as pltpu
from jax.sharding import Mesh
from jax.sharding import PartitionSpec as P


LANES = 128
SPAN = 64
PARTS = 2
DOWN_LANES = 512
TOPK = 2
PLANE = ("sp_1", "sp_2")
SP = ("sp_0", "sp_1", "sp_2")
TP = ("tp_0", "tp_1")
SP_TP = SP + TP
ROW_PAIRS = ((1, 2), (2, 1), (3, 0), (0, 3))
WEIGHT_PAIRS = ((0, 1), (1, 0), (2, 3), (3, 2))
FIRST_SHARE = (2, 3)


f32 = jnp.float32
bf16 = jnp.bfloat16
epsilon = 1e-06
exact = lax.Precision.HIGHEST


def dot(a, b, dims=((1,), (0,)), precision=None):
    return lax.dot_general(a, b, (dims, ((), ())), precision=precision, preferred_element_type=f32)


def split(value):
    high = value.astype(bf16)
    return high, (value - high.astype(f32)).astype(bf16)


def silu(value):
    return value * jax.nn.sigmoid(value)


def call(kernel, out_shape, *operands, kinds="", scratch=(), mib=12):
    spaces = {
        "v": pl.BlockSpec(memory_space=pltpu.VMEM),
        "h": pl.BlockSpec(memory_space=pltpu.HBM),
        "s": pl.BlockSpec(memory_space=pltpu.SMEM),
    }
    kinds = kinds or "v" * len(operands)
    return pl.pallas_call(
        kernel,
        out_shape=out_shape,
        in_specs=[spaces[kind] for _, kind in zip(operands, kinds, strict=True)],
        out_specs=jax.tree.map(lambda _: spaces["v"], out_shape),
        scratch_shapes=scratch,
        compiler_params=pltpu.CompilerParams(vmem_limit_bytes=mib * 1024 * 1024),
    )(*operands)


def decays(forget_ref, floor_ref, extra_ref, table):
    weight = (1.0 - floor_ref[...]) * jax.nn.sigmoid(-forget_ref[...].astype(f32))
    single = jnp.log1p(-weight)
    summed = dot(table, single, precision=exact)
    extra = extra_ref[...]
    extra_summed = dot(table, extra, ((1,), (1,)), precision=exact)
    return weight, summed, extra_summed


def state_kernel(forget_ref, value_ref, floor_ref, extra_ref, out_ref):
    rows, width = forget_ref.shape
    heads = width // LANES
    pieces = out_ref.shape[0]
    piece = LANES // pieces
    at = lax.broadcasted_iota(jnp.int32, (rows, rows), 0)
    other = lax.broadcasted_iota(jnp.int32, (rows, rows), 1)
    after = (other > at).astype(f32)
    weight, tail, extra_tail = decays(forget_ref, floor_ref, extra_ref, after)
    first = jnp.log1p(-weight[:1])
    row_at = lax.broadcasted_iota(jnp.int32, (16, LANES), 0)
    decay_rows = jnp.zeros((16, LANES), f32)
    for h in range(heads):
        lanes = slice(h * LANES, (h + 1) * LANES)
        rest = tail[:, lanes] + extra_tail[:, h : h + 1]
        total = rest[:1] + first[:, lanes] + extra_ref[h : h + 1, 0:1]
        high = total.astype(bf16).astype(f32)
        decay_rows = jnp.where(row_at == h, high, decay_rows)
        decay_rows = jnp.where(row_at == heads + h, total - high, decay_rows)
        scaled_high, scaled_low = split(weight[:, lanes] * jnp.exp(rest))
        value = value_ref[:, lanes]
        state = dot(value, scaled_high, ((0,), (0,))) + dot(value, scaled_low, ((0,), (0,)))
        for p in range(pieces):
            out_ref[p, h * piece : (h + 1) * piece, :] = state[p * piece : (p + 1) * piece].astype(bf16)
    for p in range(pieces):
        out_ref[p, heads * piece :, :] = decay_rows.astype(bf16)


def read_piece(ref, j, heads, piece):
    states = [ref[j, h * piece : (h + 1) * piece, :].astype(f32) for h in range(heads)]
    rows = ref[j, heads * piece :, :].astype(f32)
    totals = [rows[h : h + 1] + rows[heads + h : heads + h + 1] for h in range(heads)]
    return states, totals


def plane_kernel(heads, in_ref, out_ref, before_ref, passed_ref):
    members = in_ref.shape[0]
    piece = before_ref.shape[1] // heads
    running = [jnp.zeros((piece, LANES), f32) for _ in range(heads)]
    total = [jnp.zeros((1, LANES), f32) for _ in range(heads)]
    passed_ref[...] = jnp.zeros(passed_ref.shape, f32)
    for j in range(members):
        states, decay = read_piece(in_ref, j, heads, piece)
        for h in range(heads):
            before_ref[j, h * piece : (h + 1) * piece, :] = running[h]
            passed_ref[j, h : h + 1, :] = total[h]
            running[h] = jnp.exp(decay[h]) * running[h] + states[h]
            total[h] = total[h] + decay[h]
    row_at = lax.broadcasted_iota(jnp.int32, (16, LANES), 0)
    decay_rows = jnp.zeros((16, LANES), f32)
    for h in range(heads):
        high = total[h].astype(bf16).astype(f32)
        decay_rows = jnp.where(row_at == h, high, decay_rows)
        decay_rows = jnp.where(row_at == heads + h, total[h] - high, decay_rows)
    for k in range(out_ref.shape[0]):
        for h in range(heads):
            out_ref[k, h * piece : (h + 1) * piece, :] = running[h].astype(bf16)
        out_ref[k, heads * piece :, :] = decay_rows.astype(bf16)


def carry_kernel(heads, place_ref, in_ref, before_ref, passed_ref, out_ref):
    piece = before_ref.shape[1] // heads
    place = place_ref[0]
    running = [jnp.zeros((piece, LANES), f32) for _ in range(heads)]
    for k in range(in_ref.shape[0]):
        states, decay = read_piece(in_ref, k, heads, piece)
        for h in range(heads):
            following = jnp.exp(decay[h]) * running[h] + states[h]
            running[h] = jnp.where(k < place, following, running[h])
    for j in range(out_ref.shape[0]):
        for h in range(heads):
            rows = slice(h * piece, (h + 1) * piece)
            out_ref[j, rows, :] = (
                jnp.exp(passed_ref[j, h : h + 1, :]) * running[h] + before_ref[j, rows, :]
            ).astype(bf16)


def local_kernel(query_ref, forget_ref, value_ref, floor_ref, extra_ref, out_ref):
    rows, width = query_ref.shape
    at = lax.broadcasted_iota(jnp.int32, (rows, rows), 0)
    other = lax.broadcasted_iota(jnp.int32, (rows, rows), 1)
    upto = ((other <= at) & (at // SPAN == other // SPAN)).astype(f32)
    weight, summed, extra_summed = decays(forget_ref, floor_ref, extra_ref, upto)
    query = silu(query_ref[...].astype(f32))
    causal = lax.broadcasted_iota(jnp.int32, (SPAN, SPAN), 0) >= lax.broadcasted_iota(
        jnp.int32, (SPAN, SPAN), 1
    )
    for h in range(width // LANES):
        lanes = slice(h * LANES, (h + 1) * LANES)
        running = summed[:, lanes] + extra_summed[:, h : h + 1]
        asked = query[:, lanes] * jnp.exp(running)
        state = jnp.zeros((LANES, LANES), f32)
        passed = jnp.zeros((1, LANES), f32)
        for b in range(rows // SPAN):
            part = slice(b * SPAN, (b + 1) * SPAN)
            decay = running[part]
            final = decay[SPAN - 1 :]
            asked_now = asked[part].astype(bf16)
            value = value_ref[part, lanes]
            given = weight[part, lanes]
            scores = dot(asked_now, (given * jnp.exp(-decay)).astype(bf16), ((1,), (1,)))
            scores = jnp.where(causal, scores, 0.0).astype(bf16)
            out = dot(scores, value)
            if b:
                out = out + dot(asked_now, state.astype(bf16), ((1,), (1,)))
            out_ref[0, part, lanes] = out
            out_ref[1, part, lanes] = asked[part] * jnp.exp(passed)
            passed = passed + final
            kept = (given * jnp.exp(final - decay)).astype(bf16)
            state = state * jnp.exp(final) + dot(value, kept, ((0,), (0,)))


def head_kernel(local_ref, carry_ref, gain_ref, gate_ref, out_ref):
    width = local_ref.shape[2]
    heads = width // LANES
    piece = carry_ref.shape[1] // heads
    for h in range(heads):
        lanes = slice(h * LANES, (h + 1) * LANES)
        carried = jnp.concatenate(
            [carry_ref[p, h * piece : (h + 1) * piece, :] for p in range(carry_ref.shape[0])], axis=0
        )
        late = local_ref[1, :, lanes].astype(bf16)
        mixed = local_ref[0, :, lanes] + dot(late, carried, ((1,), (1,)))
        scale = lax.rsqrt(jnp.mean(mixed * mixed, axis=-1, keepdims=True) + epsilon)
        gate = silu(gate_ref[:, lanes].astype(f32))
        hidden = (mixed * scale * gain_ref[:, lanes] * gate).astype(bf16)
        for k in range(out_ref.shape[0]):
            out_ref[k, :, lanes] = hidden


def slots_in_row(column_ref, row_ref, capacity):
    tokens = column_ref.shape[0]
    earlier = lax.broadcasted_iota(jnp.int32, (tokens, tokens), 0) < lax.broadcasted_iota(
        jnp.int32, (tokens, tokens), 1
    )
    slots = []
    for j in range(TOPK):
        mine = row_ref[j : j + 1, :]
        rank = jnp.zeros((1, tokens), f32)
        for i in range(j + 1):
            same = column_ref[:, i : i + 1] == mine
            if i == j:
                same = same & earlier
            rank = rank + jnp.sum(same.astype(f32), axis=0, keepdims=True)
        slots.append(mine * (PARTS * capacity) + rank.astype(jnp.int32))
    return slots


def slots_in_column(column_ref, row_ref, capacity):
    tokens = column_ref.shape[0]
    earlier = lax.broadcasted_iota(jnp.int32, (tokens, tokens), 1) < lax.broadcasted_iota(
        jnp.int32, (tokens, tokens), 0
    )
    slots = []
    for j in range(TOPK):
        mine = column_ref[:, j : j + 1]
        rank = jnp.zeros((tokens, 1), f32)
        for i in range(j + 1):
            same = row_ref[i : i + 1, :] == mine
            if i == j:
                same = same & earlier
            rank = rank + jnp.sum(same.astype(f32), axis=1, keepdims=True)
        slots.append(mine * (PARTS * capacity) + rank.astype(jnp.int32))
    return slots


def spread_table(rows, columns, capacity, part):
    row = lax.broadcasted_iota(jnp.int32, (rows, columns), 0)
    column = lax.broadcasted_iota(jnp.int32, (rows, columns), 1)
    stride = PARTS * capacity
    wanted = (column // capacity) * stride + part * capacity + column % capacity
    return (row == wanted).astype(f32).astype(bf16)


def gather_table(rows, columns, capacity, part):
    row = lax.broadcasted_iota(jnp.int32, (rows, columns), 0)
    column = lax.broadcasted_iota(jnp.int32, (rows, columns), 1)
    stride = PARTS * capacity
    wanted = (row // capacity) * stride + part * capacity + row % capacity
    return (column == wanted).astype(f32).astype(bf16)


def dispatch_kernel(capacity, mix_ref, stream_ref, gain_ref, column_ref, row_ref, residual_ref, *send_refs):
    tokens, width = stream_ref.shape
    blocks, _, block = mix_ref.shape
    square = jnp.zeros((tokens, 1), f32)
    for k in range(blocks):
        lanes = slice(k * block, (k + 1) * block)
        residual = stream_ref[:, lanes].astype(f32) + mix_ref[k].astype(f32)
        residual_ref[:, lanes] = residual
        square = square + jnp.sum(residual * residual, axis=1, keepdims=True)
    scale = lax.rsqrt(square / width + epsilon)
    slots = slots_in_row(column_ref, row_ref, capacity)
    slot_at = lax.broadcasted_iota(jnp.int32, (send_refs[0].shape[0], tokens), 0)
    tables = [
        ((slot_at == slots[0] + q * capacity) | (slot_at == slots[1] + q * capacity))
        .astype(f32)
        .astype(bf16)
        for q in range(PARTS)
    ]
    start = 0
    for send_ref in send_refs:
        part = send_ref.shape[1]
        send = jnp.zeros(send_ref.shape, f32)
        for q in range(PARTS):
            lanes = slice(start, start + part)
            start += part
            normed = (residual_ref[:, lanes] * scale * gain_ref[:, lanes]).astype(bf16)
            send = send + dot(tables[q], normed)
        send_ref[...] = send.astype(bf16)


def gate_up(own_ref, others_ref, weight_refs, capacity):
    rows, part = own_ref.shape
    tables = [gather_table(rows // PARTS, rows, capacity, q) for q in range(PARTS)]
    laid = [
        jnp.concatenate([dot(table, ref[...]).astype(bf16) for table in tables], axis=1)
        for ref in (own_ref, others_ref)
    ]
    for j, weight_ref in enumerate(weight_refs):
        weight = weight_ref[: PARTS * part, :]
        for i in range(2):
            yield i, j, dot(laid[i], weight)


def first_kernel(
    capacity, own_ref, others_ref, gate_ref, up_ref, gate_too_ref, up_too_ref, acts_ref, kept_ref
):
    weight_refs = (gate_ref, up_ref, gate_too_ref, up_too_ref)
    for i, j, product in gate_up(own_ref, others_ref, weight_refs, capacity):
        acts_ref[i, j] = product
    left = kept_ref.shape[1]
    for j, weight_ref in enumerate(weight_refs):
        kept_ref[j] = weight_ref[weight_ref.shape[0] - left :, :]


def second_kernel(capacity, own_ref, others_ref, kept_ref, acts_ref, mine_ref, theirs_ref):
    outs = (mine_ref, theirs_ref)
    width = kept_ref.shape[2]
    gates = {}
    weight_refs = [kept_ref.at[j] for j in range(kept_ref.shape[0])]
    for i, j, product in gate_up(own_ref, others_ref, weight_refs, capacity):
        product = product + acts_ref[i, j]
        if j % 2 == 0:
            gates[i] = silu(product)
        else:
            lanes = slice(j // 2 * width, (j // 2 + 1) * width)
            outs[i][:, lanes] = (gates[i] * product).astype(bf16)


def down_kernel(capacity, mine_ref, rest_ref, *refs):
    *weight_refs, out_ref = refs
    width = weight_refs[0].shape[0]
    inner = [ref[:, k * width : (k + 1) * width] for ref in (mine_ref, rest_ref) for k in range(2)]
    rows = mine_ref.shape[0]
    block = out_ref.shape[1]
    part = weight_refs[0].shape[1] // PARTS
    out = jnp.zeros(out_ref.shape, f32)
    for q in range(PARTS):
        lanes = pl.ds(pl.multiple_of(q * part + pl.program_id(0) * block, LANES), block)
        product = dot(inner[0], weight_refs[0][:, lanes])
        for k in range(1, len(inner)):
            product = product + dot(inner[k], weight_refs[k][:, lanes])
        out = out + dot(spread_table(PARTS * rows, rows, capacity, q), product.astype(bf16))
    out_ref[...] = out.astype(bf16)


def project_down(capacity, mine, rest, weights):
    rows = mine.shape[0]
    part = weights[0].shape[1] // PARTS
    whole = pl.BlockSpec(memory_space=pltpu.VMEM)
    return pl.pallas_call(
        lambda *refs: down_kernel(capacity, *refs),
        grid=(part // DOWN_LANES,),
        out_shape=jax.ShapeDtypeStruct((PARTS * rows, part), bf16),
        in_specs=[whole, whole] + [whole for _ in weights],
        out_specs=pl.BlockSpec((PARTS * rows, DOWN_LANES), lambda k: (0, k)),
        compiler_params=pltpu.CompilerParams(vmem_limit_bytes=12 * 1024 * 1024),
    )(mine, rest, *weights)


def combine_kernel(capacity, results_ref, residual_ref, column_ref, row_ref, weight_ref, out_ref):
    tokens = residual_ref.shape[0]
    slots = slots_in_column(column_ref, row_ref, capacity)
    weight = weight_ref[...]
    weight = weight / jnp.sum(weight, axis=1, keepdims=True)
    count, part = results_ref.shape
    for q in range(PARTS):
        slot_at = lax.broadcasted_iota(jnp.int32, (tokens, count), 1) - q * capacity
        table = jnp.zeros((tokens, count), f32)
        for j in range(TOPK):
            table = table + jnp.where(slot_at == slots[j], weight[:, j : j + 1], 0.0)
        high, low = split(table)
        results = results_ref[...]
        lanes = slice(q * part, (q + 1) * part)
        routed = dot(high, results) + dot(low, results)
        out_ref[:, lanes] = (residual_ref[:, lanes] + routed).astype(bf16)


def spread(value, axes):
    return lax.all_to_all(value, axes, split_axis=0, concat_axis=0, tiled=True)


def layer(
    query,
    forget_preact,
    value_input,
    output_gate,
    forget_minimum,
    extra_log_decay,
    head_norm_gain,
    output_weight,
    stream,
    feedforward_gain,
    routes,
    router_weight,
    expert_gate_weight,
    expert_up_weight,
    expert_down_weight,
):
    window_rows, width = query.shape
    heads = width // LANES
    tp_size = lax.axis_size(TP)
    sp_size = lax.axis_size(SP)
    plane = lax.axis_size(PLANE)
    planes = lax.axis_size("sp_0")
    quarter_rows, model_width = stream.shape
    capacity = window_rows // sp_size
    piece = LANES // plane

    down = expert_down_weight[0]
    down_near = lax.ppermute(down, TP, WEIGHT_PAIRS)
    down_next = lax.ppermute(down, TP, ROW_PAIRS)

    floor = forget_minimum.reshape(1, -1)
    message = jax.ShapeDtypeStruct((plane, heads * piece + 16, LANES), bf16)
    states = call(
        state_kernel, message, forget_preact, value_input, floor, extra_log_decay
    )
    states = spread(states, PLANE)
    totals, before, passed = call(
        lambda *refs: plane_kernel(heads, *refs),
        (
            jax.ShapeDtypeStruct((planes, heads * piece + 16, LANES), bf16),
            jax.ShapeDtypeStruct((plane, heads * piece, LANES), f32),
            jax.ShapeDtypeStruct((plane, 8, LANES), f32),
        ),
        states,
    )
    totals = spread(totals, "sp_0")
    local = call(
        local_kernel,
        jax.ShapeDtypeStruct((2, window_rows, width), f32),
        query,
        forget_preact,
        value_input,
        floor,
        extra_log_decay,
    )
    place = lax.axis_index("sp_0").astype(jnp.int32).reshape(1)
    carried = call(
        lambda *refs: carry_kernel(heads, *refs),
        jax.ShapeDtypeStruct((plane, heads * piece, LANES), bf16),
        place,
        totals,
        before,
        passed,
        kinds="svvv",
    )
    carried = spread(carried, PLANE)
    hidden = call(
        head_kernel,
        jax.ShapeDtypeStruct((tp_size, window_rows, width), bf16),
        local,
        carried,
        head_norm_gain.reshape(1, -1),
        output_gate,
    )
    hidden = spread(hidden, TP)
    projected = jnp.einsum(
        "ptc,pcd->td",
        hidden,
        output_weight.reshape(tp_size, width, -1),
        preferred_element_type=f32,
    ).astype(bf16)
    gate_weight, up_weight, down_near, projected = lax.optimization_barrier(
        (expert_gate_weight[0], expert_up_weight[0], down_near, projected)
    )
    mix = spread(projected.reshape(tp_size, quarter_rows, -1), TP)
    down_far = lax.ppermute(down_near, TP, ROW_PAIRS)
    gate_weight_too = lax.ppermute(gate_weight, TP, WEIGHT_PAIRS)
    up_weight_too = lax.ppermute(up_weight, TP, WEIGHT_PAIRS)

    own = lax.dynamic_slice_in_dim(routes, lax.axis_index(TP) * quarter_rows, quarter_rows, 0)
    own_rows = own.T
    first_depth = model_width * FIRST_SHARE[0] // FIRST_SHARE[1]
    packed = [
        jax.ShapeDtypeStruct((window_rows * PARTS, depth // PARTS), bf16)
        for depth in (first_depth, model_width - first_depth)
    ]
    residual, *sends = call(
        lambda *refs: dispatch_kernel(capacity, *refs),
        (jax.ShapeDtypeStruct((quarter_rows, model_width), f32), *packed),
        mix,
        stream,
        feedforward_gain.reshape(1, -1),
        own,
        own_rows,
    )
    hidden_part = expert_gate_weight.shape[2]
    rows = []
    for send in sends:
        received = spread(send.reshape(sp_size, PARTS * capacity, -1), SP).reshape(send.shape)
        rows.append((received, lax.ppermute(received, TP, ROW_PAIRS)))
    weights = (gate_weight, up_weight, gate_weight_too, up_weight_too)
    count = len(weights)
    acts, kept = call(
        lambda *refs: first_kernel(capacity, *refs),
        (
            jax.ShapeDtypeStruct((2, count, window_rows, hidden_part), f32),
            jax.ShapeDtypeStruct((count, model_width - first_depth, hidden_part), bf16),
        ),
        *rows[0],
        *weights,
        mib=16,
    )
    acts, down_near, down_next, down_far = lax.optimization_barrier(
        (acts, down_near, down_next, down_far)
    )
    mine, theirs = call(
        lambda *refs: second_kernel(capacity, *refs),
        (jax.ShapeDtypeStruct((window_rows, 2 * hidden_part), bf16),) * 2,
        *rows[1],
        kept,
        acts,
    )
    rest = lax.ppermute(theirs, TP, ROW_PAIRS)
    expert_out = project_down(
        capacity, mine, rest, (down, down_near, down_next, down_far)
    )
    returned = spread(expert_out.reshape(sp_size, PARTS * capacity, -1), SP)
    return call(
        lambda *refs: combine_kernel(capacity, *refs),
        jax.ShapeDtypeStruct((quarter_rows, model_width), bf16),
        returned.reshape(expert_out.shape),
        residual,
        own,
        own_rows,
        router_weight,
    )


def solution(mesh):
    torus = Mesh(mesh.devices.reshape(8, 4, 2, 2, 2), SP_TP)
    placed = (
        P(SP, TP),
        P(SP, TP),
        P(SP, TP),
        P(SP, TP),
        P(TP),
        P(TP, SP),
        P(TP),
        P(None, TP),
        P(SP_TP, None),
        P(),
        P(SP, None),
        P(SP_TP, None),
        P(SP, None, TP),
        P(SP, None, TP),
        P(SP, TP, None),
    )
    return jax.shard_map(
        layer, mesh=torus, in_specs=placed, out_specs=P(SP_TP, None), check_vma=False
    )
```

```python
import jax
import jax.numpy as jnp
from jax import lax
from jax.experimental import pallas as pl
from jax.experimental.pallas import tpu as pltpu
from jax.sharding import Mesh
from jax.sharding import PartitionSpec as P


LANES = 128
SPAN = 64
PARTS = 2
DOWN_LANES = 512
TOPK = 2
PLANE = ("sp_1", "sp_2")
SP = ("sp_0", "sp_1", "sp_2")
TP = ("tp_0", "tp_1")
SP_TP = SP + TP
ROW_PAIRS = ((1, 2), (2, 1), (3, 0), (0, 3))
WEIGHT_PAIRS = ((0, 1), (1, 0), (2, 3), (3, 2))
FIRST_SHARE = (3, 4)


f32 = jnp.float32
bf16 = jnp.bfloat16
epsilon = 1e-06
exact = lax.Precision.HIGHEST


def dot(a, b, dims=((1,), (0,)), precision=None):
    return lax.dot_general(a, b, (dims, ((), ())), precision=precision, preferred_element_type=f32)


def split(value):
    high = value.astype(bf16)
    return high, (value - high.astype(f32)).astype(bf16)


def silu(value):
    return value * jax.nn.sigmoid(value)


def call(kernel, out_shape, *operands, kinds="", scratch=(), mib=12):
    spaces = {
        "v": pl.BlockSpec(memory_space=pltpu.VMEM),
        "h": pl.BlockSpec(memory_space=pltpu.HBM),
        "s": pl.BlockSpec(memory_space=pltpu.SMEM),
    }
    kinds = kinds or "v" * len(operands)
    return pl.pallas_call(
        kernel,
        out_shape=out_shape,
        in_specs=[spaces[kind] for _, kind in zip(operands, kinds, strict=True)],
        out_specs=jax.tree.map(lambda _: spaces["v"], out_shape),
        scratch_shapes=scratch,
        compiler_params=pltpu.CompilerParams(vmem_limit_bytes=mib * 1024 * 1024),
    )(*operands)


def decays(forget_ref, floor_ref, extra_ref, table):
    weight = (1.0 - floor_ref[...][None, :]) * jax.nn.sigmoid(-forget_ref[...].astype(f32))
    single = jnp.log1p(-weight)
    summed = dot(table, single, precision=exact)
    extra = extra_ref[...]
    extra_summed = dot(table, extra, ((1,), (1,)), precision=exact)
    return weight, summed, extra_summed


def state_kernel(forget_ref, value_ref, floor_ref, extra_ref, out_ref):
    rows, width = forget_ref.shape
    heads = width // LANES
    pieces = out_ref.shape[0]
    piece = LANES // pieces
    at = lax.broadcasted_iota(jnp.int32, (rows, rows), 0)
    other = lax.broadcasted_iota(jnp.int32, (rows, rows), 1)
    after = (other > at).astype(f32)
    weight, tail, extra_tail = decays(forget_ref, floor_ref, extra_ref, after)
    first = jnp.log1p(-weight[:1])
    row_at = lax.broadcasted_iota(jnp.int32, (16, LANES), 0)
    decay_rows = jnp.zeros((16, LANES), f32)
    for h in range(heads):
        lanes = slice(h * LANES, (h + 1) * LANES)
        rest = tail[:, lanes] + extra_tail[:, h : h + 1]
        total = rest[:1] + first[:, lanes] + extra_ref[h : h + 1, 0:1]
        high = total.astype(bf16).astype(f32)
        decay_rows = jnp.where(row_at == h, high, decay_rows)
        decay_rows = jnp.where(row_at == heads + h, total - high, decay_rows)
        scaled_high, scaled_low = split(weight[:, lanes] * jnp.exp(rest))
        value = value_ref[:, lanes]
        state = dot(value, scaled_high, ((0,), (0,))) + dot(value, scaled_low, ((0,), (0,)))
        for p in range(pieces):
            out_ref[p, h * piece : (h + 1) * piece, :] = state[p * piece : (p + 1) * piece].astype(bf16)
    for p in range(pieces):
        out_ref[p, heads * piece :, :] = decay_rows.astype(bf16)


def read_piece(ref, j, heads, piece):
    states = [ref[j, h * piece : (h + 1) * piece, :].astype(f32) for h in range(heads)]
    rows = ref[j, heads * piece :, :].astype(f32)
    totals = [rows[h : h + 1] + rows[heads + h : heads + h + 1] for h in range(heads)]
    return states, totals


def plane_kernel(heads, in_ref, out_ref, before_ref, passed_ref):
    members = in_ref.shape[0]
    piece = before_ref.shape[1] // heads
    running = [jnp.zeros((piece, LANES), f32) for _ in range(heads)]
    total = [jnp.zeros((1, LANES), f32) for _ in range(heads)]
    passed_ref[...] = jnp.zeros(passed_ref.shape, f32)
    for j in range(members):
        states, decay = read_piece(in_ref, j, heads, piece)
        for h in range(heads):
            before_ref[j, h * piece : (h + 1) * piece, :] = running[h]
            passed_ref[j, h : h + 1, :] = total[h]
            running[h] = jnp.exp(decay[h]) * running[h] + states[h]
            total[h] = total[h] + decay[h]
    row_at = lax.broadcasted_iota(jnp.int32, (16, LANES), 0)
    decay_rows = jnp.zeros((16, LANES), f32)
    for h in range(heads):
        high = total[h].astype(bf16).astype(f32)
        decay_rows = jnp.where(row_at == h, high, decay_rows)
        decay_rows = jnp.where(row_at == heads + h, total[h] - high, decay_rows)
    for k in range(out_ref.shape[0]):
        for h in range(heads):
            out_ref[k, h * piece : (h + 1) * piece, :] = running[h].astype(bf16)
        out_ref[k, heads * piece :, :] = decay_rows.astype(bf16)


def carry_kernel(heads, place_ref, in_ref, before_ref, passed_ref, out_ref):
    piece = before_ref.shape[1] // heads
    place = place_ref[0]
    running = [jnp.zeros((piece, LANES), f32) for _ in range(heads)]
    for k in range(in_ref.shape[0]):
        states, decay = read_piece(in_ref, k, heads, piece)
        for h in range(heads):
            following = jnp.exp(decay[h]) * running[h] + states[h]
            running[h] = jnp.where(k < place, following, running[h])
    for j in range(out_ref.shape[0]):
        for h in range(heads):
            rows = slice(h * piece, (h + 1) * piece)
            out_ref[j, rows, :] = (
                jnp.exp(passed_ref[j, h : h + 1, :]) * running[h] + before_ref[j, rows, :]
            ).astype(bf16)


def local_kernel(
    query_ref, forget_ref, value_ref, gate_ref, floor_ref, extra_ref, gain_ref, out_ref
):
    rows, width = query_ref.shape
    at = lax.broadcasted_iota(jnp.int32, (rows, rows), 0)
    other = lax.broadcasted_iota(jnp.int32, (rows, rows), 1)
    upto = ((other <= at) & (at // SPAN == other // SPAN)).astype(f32)
    weight, summed, extra_summed = decays(forget_ref, floor_ref, extra_ref, upto)
    query = silu(query_ref[...].astype(f32))
    out_ref[2] = gain_ref[...][None, :] * silu(gate_ref[...].astype(f32))
    causal = lax.broadcasted_iota(jnp.int32, (SPAN, SPAN), 0) >= lax.broadcasted_iota(
        jnp.int32, (SPAN, SPAN), 1
    )
    for h in range(width // LANES):
        lanes = slice(h * LANES, (h + 1) * LANES)
        running = summed[:, lanes] + extra_summed[:, h : h + 1]
        asked = query[:, lanes] * jnp.exp(running)
        state = jnp.zeros((LANES, LANES), f32)
        passed = jnp.zeros((1, LANES), f32)
        for b in range(rows // SPAN):
            part = slice(b * SPAN, (b + 1) * SPAN)
            decay = running[part]
            final = decay[SPAN - 1 :]
            asked_now = asked[part].astype(bf16)
            value = value_ref[part, lanes]
            given = weight[part, lanes]
            scores = dot(asked_now, (given * jnp.exp(-decay)).astype(bf16), ((1,), (1,)))
            scores = jnp.where(causal, scores, 0.0).astype(bf16)
            out = dot(scores, value)
            if b:
                out = out + dot(asked_now, state.astype(bf16), ((1,), (1,)))
            out_ref[0, part, lanes] = out
            out_ref[1, part, lanes] = asked[part] * jnp.exp(passed)
            passed = passed + final
            kept = (given * jnp.exp(final - decay)).astype(bf16)
            state = state * jnp.exp(final) + dot(value, kept, ((0,), (0,)))


def head_kernel(local_ref, carry_ref, out_ref):
    width = local_ref.shape[2]
    heads = width // LANES
    piece = carry_ref.shape[1] // heads
    for h in range(heads):
        lanes = slice(h * LANES, (h + 1) * LANES)
        carried = jnp.concatenate(
            [carry_ref[p, h * piece : (h + 1) * piece, :] for p in range(carry_ref.shape[0])], axis=0
        )
        late = local_ref[1, :, lanes].astype(bf16)
        mixed = local_ref[0, :, lanes] + dot(late, carried, ((1,), (1,)))
        scale = lax.rsqrt(jnp.mean(mixed * mixed, axis=-1, keepdims=True) + epsilon)
        out_ref[:, lanes] = (mixed * scale * local_ref[2, :, lanes]).astype(bf16)


def project_kernel(place_ref, *refs):
    count = (len(refs) - 2) // 2
    hidden_refs, (weight_ref, *out_refs, held_ref) = refs[:count], refs[count:]
    width = hidden_refs[0].shape[1]
    place = place_ref[0]
    projected = jnp.zeros(held_ref.shape, f32)
    for k, hidden_ref in enumerate(hidden_refs):
        start = pl.multiple_of((place + count - k) % count * width, width)
        projected = projected + dot(hidden_ref[...], weight_ref[pl.ds(start, width), :])
    held_ref[...] = projected
    for k, out_ref in enumerate(out_refs):
        tokens = out_ref.shape[0]
        start = pl.multiple_of((place + k) % count * tokens, tokens)
        out_ref[...] = held_ref[pl.ds(start, tokens), :].astype(bf16)


def slots_in_row(column_ref, row_ref, capacity):
    tokens = column_ref.shape[0]
    earlier = lax.broadcasted_iota(jnp.int32, (tokens, tokens), 0) < lax.broadcasted_iota(
        jnp.int32, (tokens, tokens), 1
    )
    slots = []
    for j in range(TOPK):
        mine = row_ref[j : j + 1, :]
        rank = jnp.zeros((1, tokens), f32)
        for i in range(j + 1):
            same = column_ref[:, i : i + 1] == mine
            if i == j:
                same = same & earlier
            rank = rank + jnp.sum(same.astype(f32), axis=0, keepdims=True)
        slots.append(mine * (PARTS * capacity) + rank.astype(jnp.int32))
    return slots


def slots_in_column(column_ref, row_ref, capacity):
    tokens = column_ref.shape[0]
    earlier = lax.broadcasted_iota(jnp.int32, (tokens, tokens), 1) < lax.broadcasted_iota(
        jnp.int32, (tokens, tokens), 0
    )
    slots = []
    for j in range(TOPK):
        mine = column_ref[:, j : j + 1]
        rank = jnp.zeros((tokens, 1), f32)
        for i in range(j + 1):
            same = row_ref[i : i + 1, :] == mine
            if i == j:
                same = same & earlier
            rank = rank + jnp.sum(same.astype(f32), axis=1, keepdims=True)
        slots.append(mine * (PARTS * capacity) + rank.astype(jnp.int32))
    return slots


def spread_table(rows, columns, capacity, part):
    row = lax.broadcasted_iota(jnp.int32, (rows, columns), 0)
    column = lax.broadcasted_iota(jnp.int32, (rows, columns), 1)
    stride = PARTS * capacity
    wanted = (column // capacity) * stride + part * capacity + column % capacity
    return (row == wanted).astype(f32).astype(bf16)


def gather_table(rows, columns, capacity, part):
    row = lax.broadcasted_iota(jnp.int32, (rows, columns), 0)
    column = lax.broadcasted_iota(jnp.int32, (rows, columns), 1)
    stride = PARTS * capacity
    wanted = (row // capacity) * stride + part * capacity + row % capacity
    return (column == wanted).astype(f32).astype(bf16)


def dispatch_kernel(capacity, place_ref, *refs):
    *refs, mix_ref = refs
    blocks, _, block = mix_ref.shape
    for k in range(blocks):
        mix_ref[(place_ref[0] + blocks - k) % blocks] = refs[k][...]
    stream_ref, gain_ref, column_ref, row_ref, residual_ref, *send_refs = refs[blocks:]
    tokens, width = stream_ref.shape
    square = jnp.zeros((tokens, 1), f32)
    for k in range(blocks):
        lanes = slice(k * block, (k + 1) * block)
        residual = stream_ref[:, lanes].astype(f32) + mix_ref[k].astype(f32)
        residual_ref[:, lanes] = residual
        square = square + jnp.sum(residual * residual, axis=1, keepdims=True)
    scale = lax.rsqrt(square / width + epsilon)
    slots = slots_in_row(column_ref, row_ref, capacity)
    slot_at = lax.broadcasted_iota(jnp.int32, (send_refs[0].shape[0], tokens), 0)
    tables = [
        ((slot_at == slots[0] + q * capacity) | (slot_at == slots[1] + q * capacity))
        .astype(f32)
        .astype(bf16)
        for q in range(PARTS)
    ]
    start = 0
    for send_ref in send_refs:
        part = send_ref.shape[1]
        send = jnp.zeros(send_ref.shape, f32)
        for q in range(PARTS):
            lanes = slice(start, start + part)
            start += part
            normed = (residual_ref[:, lanes] * scale * gain_ref[:, lanes]).astype(bf16)
            send = send + dot(tables[q], normed)
        send_ref[...] = send.astype(bf16)


def first_kernel(
    capacity, own_ref, others_ref, gate_ref, up_ref, gate_too_ref, up_too_ref, acts_ref, kept_ref
):
    weight_refs = (gate_ref, up_ref, gate_too_ref, up_too_ref)
    left = kept_ref.shape[1]
    for i, ref in enumerate((own_ref, others_ref)):
        rows = laid_out(ref, capacity)
        for j, weight_ref in enumerate(weight_refs):
            acts_ref[i, j] = dot(rows, weight_ref[: weight_ref.shape[0] - left, :])
    for j, weight_ref in enumerate(weight_refs):
        kept_ref[j] = weight_ref[weight_ref.shape[0] - left :, :]


def laid_out(received_ref, capacity):
    rows = received_ref.shape[0]
    tables = [gather_table(rows // PARTS, rows, capacity, q) for q in range(PARTS)]
    received = received_ref[...]
    return jnp.concatenate([dot(table, received).astype(bf16) for table in tables], axis=1)


def inner_of(rows, kept_ref, acts_ref, out_ref):
    width = kept_ref.shape[2]
    for j in range(kept_ref.shape[0] // 2):
        gate = acts_ref[2 * j] + dot(rows, kept_ref[2 * j])
        up = acts_ref[2 * j + 1] + dot(rows, kept_ref[2 * j + 1])
        out_ref[:, j * width : (j + 1) * width] = (silu(gate) * up).astype(bf16)


def others_kernel(capacity, others_ref, kept_ref, acts_ref, out_ref):
    inner_of(laid_out(others_ref, capacity), kept_ref, acts_ref.at[1], out_ref)


def own_kernel(capacity, own_ref, kept_ref, acts_ref, down_ref, near_ref, out_ref, inner_ref):
    inner_of(laid_out(own_ref, capacity), kept_ref, acts_ref.at[0], inner_ref)
    width = down_ref.shape[0]
    out_ref[...] = dot(inner_ref[:, :width], down_ref[...]) + dot(inner_ref[:, width:], near_ref[...])


def down_kernel(capacity, partial_ref, rest_ref, next_ref, far_ref, out_ref):
    rows, depth = rest_ref.shape
    block = out_ref.shape[1]
    part = next_ref.shape[1] // PARTS
    out = jnp.zeros(out_ref.shape, f32)
    for q in range(PARTS):
        lanes = pl.ds(pl.multiple_of(q * part + pl.program_id(0) * block, LANES), block)
        product = partial_ref[:, lanes] + dot(rest_ref[:, : depth // 2], next_ref[:, lanes])
        product = product + dot(rest_ref[:, depth // 2 :], far_ref[:, lanes])
        out = out + dot(spread_table(PARTS * rows, rows, capacity, q), product.astype(bf16))
    out_ref[...] = out.astype(bf16)


def project_down(capacity, partial, rest, weights):
    rows, width = partial.shape
    whole = pl.BlockSpec(memory_space=pltpu.VMEM)
    return pl.pallas_call(
        lambda *refs: down_kernel(capacity, *refs),
        grid=(width // PARTS // DOWN_LANES,),
        out_shape=jax.ShapeDtypeStruct((PARTS * rows, width // PARTS), bf16),
        in_specs=[whole, whole] + [whole for _ in weights],
        out_specs=pl.BlockSpec((PARTS * rows, DOWN_LANES), lambda k: (0, k)),
        compiler_params=pltpu.CompilerParams(vmem_limit_bytes=12 * 1024 * 1024),
    )(partial, rest, *weights)


def combine_kernel(
    capacity, results_ref, residual_ref, column_ref, row_ref, weight_ref, out_ref, held_ref, arrived
):
    pieces, count, width = held_ref.shape
    copies = [
        pltpu.make_async_copy(
            results_ref.at[:, k * width : (k + 1) * width], held_ref.at[k], arrived.at[k]
        )
        for k in range(pieces)
    ]
    for copy in copies:
        copy.start()
    tokens = residual_ref.shape[0]
    slots = slots_in_column(column_ref, row_ref, capacity)
    weight = weight_ref[...]
    weight = weight / jnp.sum(weight, axis=1, keepdims=True)
    tables = []
    for q in range(PARTS):
        slot_at = lax.broadcasted_iota(jnp.int32, (tokens, count), 1) - q * capacity
        table = jnp.zeros((tokens, count), f32)
        for j in range(TOPK):
            table = table + jnp.where(slot_at == slots[j], weight[:, j : j + 1], 0.0)
        tables.extend(split(table))
    table = jnp.concatenate(tables, axis=0)
    for k, copy in enumerate(copies):
        copy.wait()
        routed = dot(table, held_ref[k])
        for q in range(PARTS):
            start = (q * pieces + k) * width
            lanes = slice(start, start + width)
            high, low = (routed[(2 * q + i) * tokens : (2 * q + i + 1) * tokens] for i in range(2))
            out_ref[:, lanes] = (residual_ref[:, lanes] + (high + low)).astype(bf16)


def spread(value, axes):
    return lax.all_to_all(value, axes, split_axis=0, concat_axis=0, tiled=True)


def shifted(value, k):
    count = lax.axis_size(TP)
    return lax.ppermute(value, TP, [(i, (i + k) % count) for i in range(count)])


def layer(
    query,
    forget_preact,
    value_input,
    output_gate,
    forget_minimum,
    extra_log_decay,
    head_norm_gain,
    output_weight,
    stream,
    feedforward_gain,
    routes,
    router_weight,
    expert_gate_weight,
    expert_up_weight,
    expert_down_weight,
):
    window_rows, width = query.shape
    heads = width // LANES
    tp_size = lax.axis_size(TP)
    sp_size = lax.axis_size(SP)
    plane = lax.axis_size(PLANE)
    planes = lax.axis_size("sp_0")
    quarter_rows, model_width = stream.shape
    capacity = window_rows // sp_size
    piece = LANES // plane

    place, tp_place, down = lax.optimization_barrier(
        (
            lax.axis_index("sp_0").astype(jnp.int32).reshape(1),
            lax.axis_index(TP).astype(jnp.int32).reshape(1),
            expert_down_weight[0],
        )
    )
    down_near = lax.ppermute(down, TP, WEIGHT_PAIRS)
    down_next = lax.ppermute(down, TP, ROW_PAIRS)

    floor = forget_minimum
    message = jax.ShapeDtypeStruct((plane, heads * piece + 16, LANES), bf16)
    states = call(
        state_kernel, message, forget_preact, value_input, floor, extra_log_decay
    )
    states = spread(states, PLANE)
    totals, before, passed = call(
        lambda *refs: plane_kernel(heads, *refs),
        (
            jax.ShapeDtypeStruct((planes, heads * piece + 16, LANES), bf16),
            jax.ShapeDtypeStruct((plane, heads * piece, LANES), f32),
            jax.ShapeDtypeStruct((plane, 8, LANES), f32),
        ),
        states,
    )
    totals = spread(totals, "sp_0")
    local = call(
        local_kernel,
        jax.ShapeDtypeStruct((3, window_rows, width), f32),
        query,
        forget_preact,
        value_input,
        output_gate,
        floor,
        extra_log_decay,
        head_norm_gain,
    )
    carried = call(
        lambda *refs: carry_kernel(heads, *refs),
        jax.ShapeDtypeStruct((plane, heads * piece, LANES), bf16),
        place,
        totals,
        before,
        passed,
        kinds="svvv",
    )
    carried = spread(carried, PLANE)
    hidden = call(
        head_kernel,
        jax.ShapeDtypeStruct((window_rows, width), bf16),
        local,
        carried,
    )
    hidden = [hidden] + [shifted(hidden, k) for k in range(1, tp_size)]
    columns = output_weight.shape[1]
    projected = call(
        project_kernel,
        (jax.ShapeDtypeStruct((quarter_rows, columns), bf16),) * tp_size,
        tp_place,
        *hidden,
        output_weight,
        kinds="s" + "v" * (tp_size + 1),
        scratch=(pltpu.VMEM((window_rows, columns), f32),),
    )
    gate_weight, up_weight, down_near, projected = lax.optimization_barrier(
        (expert_gate_weight[0], expert_up_weight[0], down_near, projected)
    )
    mix = [projected[0]]
    for k in range(1, tp_size):
        mix.append(shifted(projected[k], k))
    down_far = lax.ppermute(down_near, TP, ROW_PAIRS)
    gate_weight_too = lax.ppermute(gate_weight, TP, WEIGHT_PAIRS)
    up_weight_too = lax.ppermute(up_weight, TP, WEIGHT_PAIRS)

    own = lax.dynamic_slice_in_dim(routes, lax.axis_index(TP) * quarter_rows, quarter_rows, 0)
    own_rows = own.T
    first_depth = model_width * FIRST_SHARE[0] // FIRST_SHARE[1]
    packed = [
        jax.ShapeDtypeStruct((window_rows * PARTS, depth // PARTS), bf16)
        for depth in (first_depth, model_width - first_depth)
    ]
    residual, *sends = call(
        lambda *refs: dispatch_kernel(capacity, *refs),
        (jax.ShapeDtypeStruct((quarter_rows, model_width), f32), *packed),
        tp_place,
        *mix,
        stream,
        feedforward_gain.reshape(1, -1),
        own,
        own_rows,
        kinds="s" + "v" * (tp_size + 4),
        scratch=(pltpu.VMEM((tp_size, quarter_rows, columns), bf16),),
    )
    hidden_part = expert_gate_weight.shape[2]
    rows = []
    for send in sends:
        received = spread(send.reshape(sp_size, PARTS * capacity, -1), SP).reshape(send.shape)
        rows.append((received, lax.ppermute(received, TP, ROW_PAIRS)))
    weights = (gate_weight, up_weight, gate_weight_too, up_weight_too)
    count = len(weights)
    first_rows, down_next, down_far = lax.optimization_barrier((rows[0], down_next, down_far))
    acts, kept = call(
        lambda *refs: first_kernel(capacity, *refs),
        (
            jax.ShapeDtypeStruct((2, count, window_rows, hidden_part), f32),
            jax.ShapeDtypeStruct((count, model_width - first_depth, hidden_part), bf16),
        ),
        *first_rows,
        *weights,
        mib=16,
    )
    theirs = call(
        lambda *refs: others_kernel(capacity, *refs),
        jax.ShapeDtypeStruct((window_rows, 2 * hidden_part), bf16),
        rows[1][1],
        kept,
        acts,
    )
    rest = lax.ppermute(theirs, TP, ROW_PAIRS)
    partial = call(
        lambda *refs: own_kernel(capacity, *refs),
        jax.ShapeDtypeStruct((window_rows, model_width), f32),
        rows[1][0],
        kept,
        acts,
        down,
        down_near,
        scratch=(pltpu.VMEM((window_rows, 2 * hidden_part), bf16),),
    )
    expert_out = project_down(capacity, partial, rest, (down_next, down_far))
    returned = spread(expert_out.reshape(sp_size, PARTS * capacity, -1), SP)
    return call(
        lambda *refs: combine_kernel(capacity, *refs),
        jax.ShapeDtypeStruct((quarter_rows, model_width), bf16),
        returned.reshape(expert_out.shape),
        residual,
        own,
        own_rows,
        router_weight,
        kinds="hvvvv",
        scratch=(
            pltpu.VMEM((4, expert_out.shape[0], expert_out.shape[1] // 4), bf16),
            pltpu.SemaphoreType.DMA((4,)),
        ),
    )


def solution(mesh):
    torus = Mesh(mesh.devices.reshape(8, 4, 2, 2, 2), SP_TP)
    placed = (
        P(SP, TP),
        P(SP, TP),
        P(SP, TP),
        P(SP, TP),
        P(TP),
        P(TP, SP),
        P(TP),
        P(None, TP),
        P(SP_TP, None),
        P(),
        P(SP, None),
        P(SP_TP, None),
        P(SP, None, TP),
        P(SP, None, TP),
        P(SP, TP, None),
    )
    return jax.shard_map(
        layer, mesh=torus, in_specs=placed, out_specs=P(SP_TP, None), check_vma=False
    )
```

```python
import jax
import jax.numpy as jnp
from jax import lax
from jax.experimental import pallas as pl
from jax.experimental.pallas import tpu as pltpu
from jax.sharding import Mesh
from jax.sharding import PartitionSpec as P


LANES = 128
SPAN = 64
PARTS = 2
DOWN_LANES = 512
TOPK = 2
PLANE = ("sp_1", "sp_2")
SP = ("sp_0", "sp_1", "sp_2")
TP = ("tp_0", "tp_1")
SP_TP = SP + TP
CORE_TP = ("sp_2",) + TP
EVEN_LINKS = ((0, 1), (1, 0), (2, 3), (3, 2))
ODD_LINKS = ((1, 2), (2, 1), (3, 0), (0, 3))


def by_core(first, second):
    return first + tuple((a + 4, b + 4) for a, b in second)


WEIGHT_PAIRS = by_core(EVEN_LINKS, ODD_LINKS)
ROW_PAIRS = by_core(ODD_LINKS, EVEN_LINKS)
FIRST_SHARE = (3, 4)


f32 = jnp.float32
bf16 = jnp.bfloat16
epsilon = 1e-06
exact = lax.Precision.HIGHEST


def dot(a, b, dims=((1,), (0,)), precision=None):
    return lax.dot_general(a, b, (dims, ((), ())), precision=precision, preferred_element_type=f32)


def split(value):
    high = value.astype(bf16)
    return high, (value - high.astype(f32)).astype(bf16)


def silu(value):
    return value * jax.nn.sigmoid(value)


def call(kernel, out_shape, *operands, kinds="", scratch=(), mib=12):
    spaces = {
        "v": pl.BlockSpec(memory_space=pltpu.VMEM),
        "h": pl.BlockSpec(memory_space=pltpu.HBM),
        "s": pl.BlockSpec(memory_space=pltpu.SMEM),
    }
    kinds = kinds or "v" * len(operands)
    return pl.pallas_call(
        kernel,
        out_shape=out_shape,
        in_specs=[spaces[kind] for _, kind in zip(operands, kinds, strict=True)],
        out_specs=jax.tree.map(lambda _: spaces["v"], out_shape),
        scratch_shapes=scratch,
        compiler_params=pltpu.CompilerParams(vmem_limit_bytes=mib * 1024 * 1024),
    )(*operands)


def decays(forget_ref, floor_ref, extra_ref, table):
    weight = (1.0 - floor_ref[...][None, :]) * jax.nn.sigmoid(-forget_ref[...].astype(f32))
    single = jnp.log1p(-weight)
    summed = dot(table, single, precision=exact)
    extra = extra_ref[...]
    extra_summed = dot(table, extra, ((1,), (1,)), precision=exact)
    return weight, summed, extra_summed


def state_kernel(forget_ref, value_ref, floor_ref, extra_ref, out_ref):
    rows, width = forget_ref.shape
    heads = width // LANES
    pieces = out_ref.shape[0]
    piece = LANES // pieces
    at = lax.broadcasted_iota(jnp.int32, (rows, rows), 0)
    other = lax.broadcasted_iota(jnp.int32, (rows, rows), 1)
    after = (other > at).astype(f32)
    weight, tail, extra_tail = decays(forget_ref, floor_ref, extra_ref, after)
    first = jnp.log1p(-weight[:1])
    row_at = lax.broadcasted_iota(jnp.int32, (16, LANES), 0)
    decay_rows = jnp.zeros((16, LANES), f32)
    for h in range(heads):
        lanes = slice(h * LANES, (h + 1) * LANES)
        rest = tail[:, lanes] + extra_tail[:, h : h + 1]
        total = rest[:1] + first[:, lanes] + extra_ref[h : h + 1, 0:1]
        high = total.astype(bf16).astype(f32)
        decay_rows = jnp.where(row_at == h, high, decay_rows)
        decay_rows = jnp.where(row_at == heads + h, total - high, decay_rows)
        scaled_high, scaled_low = split(weight[:, lanes] * jnp.exp(rest))
        value = value_ref[:, lanes]
        state = dot(value, scaled_high, ((0,), (0,))) + dot(value, scaled_low, ((0,), (0,)))
        for p in range(pieces):
            out_ref[p, h * piece : (h + 1) * piece, :] = state[p * piece : (p + 1) * piece].astype(bf16)
    for p in range(pieces):
        out_ref[p, heads * piece :, :] = decay_rows.astype(bf16)


def read_piece(ref, j, heads, piece):
    states = [ref[j, h * piece : (h + 1) * piece, :].astype(f32) for h in range(heads)]
    rows = ref[j, heads * piece :, :].astype(f32)
    totals = [rows[h : h + 1] + rows[heads + h : heads + h + 1] for h in range(heads)]
    return states, totals


def plane_kernel(heads, in_ref, out_ref, before_ref, passed_ref):
    members = in_ref.shape[0]
    piece = before_ref.shape[1] // heads
    running = [jnp.zeros((piece, LANES), f32) for _ in range(heads)]
    total = [jnp.zeros((1, LANES), f32) for _ in range(heads)]
    passed_ref[...] = jnp.zeros(passed_ref.shape, f32)
    for j in range(members):
        states, decay = read_piece(in_ref, j, heads, piece)
        for h in range(heads):
            before_ref[j, h * piece : (h + 1) * piece, :] = running[h]
            passed_ref[j, h : h + 1, :] = total[h]
            running[h] = jnp.exp(decay[h]) * running[h] + states[h]
            total[h] = total[h] + decay[h]
    row_at = lax.broadcasted_iota(jnp.int32, (16, LANES), 0)
    decay_rows = jnp.zeros((16, LANES), f32)
    for h in range(heads):
        high = total[h].astype(bf16).astype(f32)
        decay_rows = jnp.where(row_at == h, high, decay_rows)
        decay_rows = jnp.where(row_at == heads + h, total[h] - high, decay_rows)
    for k in range(out_ref.shape[0]):
        for h in range(heads):
            out_ref[k, h * piece : (h + 1) * piece, :] = running[h].astype(bf16)
        out_ref[k, heads * piece :, :] = decay_rows.astype(bf16)


def carry_kernel(heads, place_ref, in_ref, before_ref, passed_ref, out_ref):
    piece = before_ref.shape[1] // heads
    place = place_ref[0]
    running = [jnp.zeros((piece, LANES), f32) for _ in range(heads)]
    for k in range(in_ref.shape[0]):
        states, decay = read_piece(in_ref, k, heads, piece)
        for h in range(heads):
            following = jnp.exp(decay[h]) * running[h] + states[h]
            running[h] = jnp.where(k < place, following, running[h])
    for j in range(out_ref.shape[0]):
        for h in range(heads):
            rows = slice(h * piece, (h + 1) * piece)
            out_ref[j, rows, :] = (
                jnp.exp(passed_ref[j, h : h + 1, :]) * running[h] + before_ref[j, rows, :]
            ).astype(bf16)


def local_kernel(
    query_ref, forget_ref, value_ref, gate_ref, floor_ref, extra_ref, gain_ref, out_ref
):
    rows, width = query_ref.shape
    at = lax.broadcasted_iota(jnp.int32, (rows, rows), 0)
    other = lax.broadcasted_iota(jnp.int32, (rows, rows), 1)
    upto = ((other <= at) & (at // SPAN == other // SPAN)).astype(f32)
    weight, summed, extra_summed = decays(forget_ref, floor_ref, extra_ref, upto)
    query = silu(query_ref[...].astype(f32))
    out_ref[2] = gain_ref[...][None, :] * silu(gate_ref[...].astype(f32))
    causal = lax.broadcasted_iota(jnp.int32, (SPAN, SPAN), 0) >= lax.broadcasted_iota(
        jnp.int32, (SPAN, SPAN), 1
    )
    for h in range(width // LANES):
        lanes = slice(h * LANES, (h + 1) * LANES)
        running = summed[:, lanes] + extra_summed[:, h : h + 1]
        asked = query[:, lanes] * jnp.exp(running)
        state = jnp.zeros((LANES, LANES), f32)
        passed = jnp.zeros((1, LANES), f32)
        for b in range(rows // SPAN):
            part = slice(b * SPAN, (b + 1) * SPAN)
            decay = running[part]
            final = decay[SPAN - 1 :]
            asked_now = asked[part].astype(bf16)
            value = value_ref[part, lanes]
            given = weight[part, lanes]
            scores = dot(asked_now, (given * jnp.exp(-decay)).astype(bf16), ((1,), (1,)))
            scores = jnp.where(causal, scores, 0.0).astype(bf16)
            out = dot(scores, value)
            if b:
                out = out + dot(asked_now, state.astype(bf16), ((1,), (1,)))
            out_ref[0, part, lanes] = out
            out_ref[1, part, lanes] = asked[part] * jnp.exp(passed)
            passed = passed + final
            kept = (given * jnp.exp(final - decay)).astype(bf16)
            state = state * jnp.exp(final) + dot(value, kept, ((0,), (0,)))


def head_kernel(local_ref, carry_ref, out_ref):
    width = local_ref.shape[2]
    heads = width // LANES
    piece = carry_ref.shape[1] // heads
    for h in range(heads):
        lanes = slice(h * LANES, (h + 1) * LANES)
        carried = jnp.concatenate(
            [carry_ref[p, h * piece : (h + 1) * piece, :] for p in range(carry_ref.shape[0])], axis=0
        )
        late = local_ref[1, :, lanes].astype(bf16)
        mixed = local_ref[0, :, lanes] + dot(late, carried, ((1,), (1,)))
        scale = lax.rsqrt(jnp.mean(mixed * mixed, axis=-1, keepdims=True) + epsilon)
        out_ref[:, lanes] = (mixed * scale * local_ref[2, :, lanes]).astype(bf16)


def project_kernel(place_ref, *refs):
    count = (len(refs) - 2) // 2
    hidden_refs, (weight_ref, *out_refs, held_ref) = refs[:count], refs[count:]
    width = hidden_refs[0].shape[1]
    place = place_ref[0]
    projected = jnp.zeros(held_ref.shape, f32)
    for k, hidden_ref in enumerate(hidden_refs):
        start = pl.multiple_of((place + count - k) % count * width, width)
        projected = projected + dot(hidden_ref[...], weight_ref[pl.ds(start, width), :])
    held_ref[...] = projected
    for k, out_ref in enumerate(out_refs):
        tokens = out_ref.shape[0]
        start = pl.multiple_of((place + k) % count * tokens, tokens)
        out_ref[...] = held_ref[pl.ds(start, tokens), :].astype(bf16)


def slots_in_row(column_ref, row_ref, capacity):
    tokens = column_ref.shape[0]
    earlier = lax.broadcasted_iota(jnp.int32, (tokens, tokens), 0) < lax.broadcasted_iota(
        jnp.int32, (tokens, tokens), 1
    )
    slots = []
    for j in range(TOPK):
        mine = row_ref[j : j + 1, :]
        rank = jnp.zeros((1, tokens), f32)
        for i in range(j + 1):
            same = column_ref[:, i : i + 1] == mine
            if i == j:
                same = same & earlier
            rank = rank + jnp.sum(same.astype(f32), axis=0, keepdims=True)
        slots.append(mine * (PARTS * capacity) + rank.astype(jnp.int32))
    return slots


def slots_in_column(column_ref, row_ref, capacity):
    tokens = column_ref.shape[0]
    earlier = lax.broadcasted_iota(jnp.int32, (tokens, tokens), 1) < lax.broadcasted_iota(
        jnp.int32, (tokens, tokens), 0
    )
    slots = []
    for j in range(TOPK):
        mine = column_ref[:, j : j + 1]
        rank = jnp.zeros((tokens, 1), f32)
        for i in range(j + 1):
            same = row_ref[i : i + 1, :] == mine
            if i == j:
                same = same & earlier
            rank = rank + jnp.sum(same.astype(f32), axis=1, keepdims=True)
        slots.append(mine * (PARTS * capacity) + rank.astype(jnp.int32))
    return slots


def spread_table(rows, columns, capacity, part):
    row = lax.broadcasted_iota(jnp.int32, (rows, columns), 0)
    column = lax.broadcasted_iota(jnp.int32, (rows, columns), 1)
    stride = PARTS * capacity
    wanted = (column // capacity) * stride + part * capacity + column % capacity
    return (row == wanted).astype(f32).astype(bf16)


def gather_table(rows, columns, capacity, part):
    row = lax.broadcasted_iota(jnp.int32, (rows, columns), 0)
    column = lax.broadcasted_iota(jnp.int32, (rows, columns), 1)
    stride = PARTS * capacity
    wanted = (row // capacity) * stride + part * capacity + row % capacity
    return (column == wanted).astype(f32).astype(bf16)


def dispatch_kernel(capacity, place_ref, *refs):
    *refs, mix_ref = refs
    blocks, _, block = mix_ref.shape
    for k in range(blocks):
        mix_ref[(place_ref[0] + blocks - k) % blocks] = refs[k][...]
    stream_ref, gain_ref, column_ref, row_ref, residual_ref, *send_refs = refs[blocks:]
    tokens, width = stream_ref.shape
    square = jnp.zeros((tokens, 1), f32)
    for k in range(blocks):
        lanes = slice(k * block, (k + 1) * block)
        residual = stream_ref[:, lanes].astype(f32) + mix_ref[k].astype(f32)
        residual_ref[:, lanes] = residual
        square = square + jnp.sum(residual * residual, axis=1, keepdims=True)
    scale = lax.rsqrt(square / width + epsilon)
    slots = slots_in_row(column_ref, row_ref, capacity)
    slot_at = lax.broadcasted_iota(jnp.int32, (send_refs[0].shape[0], tokens), 0)
    tables = [
        ((slot_at == slots[0] + q * capacity) | (slot_at == slots[1] + q * capacity))
        .astype(f32)
        .astype(bf16)
        for q in range(PARTS)
    ]
    start = 0
    for send_ref in send_refs:
        part = send_ref.shape[1]
        send = jnp.zeros(send_ref.shape, f32)
        for q in range(PARTS):
            lanes = slice(start, start + part)
            start += part
            normed = (residual_ref[:, lanes] * scale * gain_ref[:, lanes]).astype(bf16)
            send = send + dot(tables[q], normed)
        send_ref[...] = send.astype(bf16)


def first_kernel(capacity, own_ref, others_ref, *refs):
    *weight_refs, acts_ref, kept_ref = refs
    depth = weight_refs[0].shape[0] - kept_ref.shape[1]
    for i, ref in enumerate((own_ref, others_ref)):
        rows = laid_out(ref, capacity)
        for j, weight_ref in enumerate(weight_refs):
            acts_ref[i, j] = dot(rows, weight_ref[:depth, :])
    for j, weight_ref in enumerate(weight_refs):
        kept_ref[j] = weight_ref[depth:, :]


def laid_out(received_ref, capacity):
    rows = received_ref.shape[0]
    tables = [gather_table(rows // PARTS, rows, capacity, q) for q in range(PARTS)]
    received = received_ref[...]
    return jnp.concatenate([dot(table, received).astype(bf16) for table in tables], axis=1)


def inner_of(rows, kept_ref, acts_ref, out_ref):
    width = kept_ref.shape[2]
    for j in range(kept_ref.shape[0] // 2):
        gate = acts_ref[2 * j] + dot(rows, kept_ref[2 * j])
        up = acts_ref[2 * j + 1] + dot(rows, kept_ref[2 * j + 1])
        out_ref[:, j * width : (j + 1) * width] = (silu(gate) * up).astype(bf16)


def others_kernel(capacity, others_ref, kept_ref, acts_ref, out_ref):
    inner_of(laid_out(others_ref, capacity), kept_ref, acts_ref.at[1], out_ref)


def own_kernel(capacity, own_ref, kept_ref, acts_ref, down_ref, near_ref, out_ref, inner_ref):
    inner_of(laid_out(own_ref, capacity), kept_ref, acts_ref.at[0], inner_ref)
    width = down_ref.shape[0]
    out_ref[...] = dot(inner_ref[:, :width], down_ref[...]) + dot(inner_ref[:, width:], near_ref[...])


def down_kernel(capacity, partial_ref, rest_ref, next_ref, far_ref, out_ref, held_ref, arrived):
    rows, depth = rest_ref.shape
    _, pieces, _, block = held_ref.shape
    each = pieces // PARTS
    order = [q * each + k for k in range(each) for q in range(PARTS)]
    copies = {
        (i, n): pltpu.make_async_copy(
            ref.at[:, n * block : (n + 1) * block], held_ref.at[i, n], arrived.at[i, n]
        )
        for n in order
        for i, ref in enumerate((next_ref, far_ref))
    }
    for copy in copies.values():
        copy.start()
    tables = [spread_table(PARTS * rows, rows, capacity, q) for q in range(PARTS)]
    rest = [rest_ref[:, : depth // 2], rest_ref[:, depth // 2 :]]
    for k in range(each):
        out = jnp.zeros((PARTS * rows, block), f32)
        for q in range(PARTS):
            n = q * each + k
            product = partial_ref[:, n * block : (n + 1) * block]
            for i in range(2):
                copies[i, n].wait()
                product = product + dot(rest[i], held_ref[i, n])
            out = out + dot(tables[q], product.astype(bf16))
        out_ref[:, k * block : (k + 1) * block] = out.astype(bf16)


def tables_kernel(capacity, column_ref, row_ref, weight_ref, out_ref):
    tokens = column_ref.shape[0]
    count = out_ref.shape[1]
    slots = slots_in_column(column_ref, row_ref, capacity)
    weight = weight_ref[...]
    weight = weight / jnp.sum(weight, axis=1, keepdims=True)
    for q in range(PARTS):
        slot_at = lax.broadcasted_iota(jnp.int32, (tokens, count), 1) - q * capacity
        table = jnp.zeros((tokens, count), f32)
        for j in range(TOPK):
            table = table + jnp.where(slot_at == slots[j], weight[:, j : j + 1], 0.0)
        for i, piece in enumerate(split(table)):
            out_ref[(2 * q + i) * tokens : (2 * q + i + 1) * tokens, :] = piece


def combine_kernel(results_ref, residual_ref, table_ref, out_ref, held_ref, arrived):
    pieces, _, width = held_ref.shape
    copies = [
        pltpu.make_async_copy(
            results_ref.at[:, k * width : (k + 1) * width], held_ref.at[k], arrived.at[k]
        )
        for k in range(pieces)
    ]
    for copy in copies:
        copy.start()
    tokens = residual_ref.shape[0]
    for k, copy in enumerate(copies):
        copy.wait()
        routed = dot(table_ref[...], held_ref[k])
        for q in range(PARTS):
            start = (q * pieces + k) * width
            lanes = slice(start, start + width)
            high, low = (routed[(2 * q + i) * tokens : (2 * q + i + 1) * tokens] for i in range(2))
            out_ref[:, lanes] = (residual_ref[:, lanes] + (high + low)).astype(bf16)


def spread(value, axes):
    return lax.all_to_all(value, axes, split_axis=0, concat_axis=0, tiled=True)


def shifted(value, k):
    count = lax.axis_size(TP)
    return lax.ppermute(value, TP, [(i, (i + k) % count) for i in range(count)])


def layer(
    query,
    forget_preact,
    value_input,
    output_gate,
    forget_minimum,
    extra_log_decay,
    head_norm_gain,
    output_weight,
    stream,
    feedforward_gain,
    routes,
    router_weight,
    expert_gate_weight,
    expert_up_weight,
    expert_down_weight,
):
    window_rows, width = query.shape
    heads = width // LANES
    tp_size = lax.axis_size(TP)
    sp_size = lax.axis_size(SP)
    plane = lax.axis_size(PLANE)
    planes = lax.axis_size("sp_0")
    quarter_rows, model_width = stream.shape
    capacity = window_rows // sp_size
    piece = LANES // plane

    place, tp_place, down = lax.optimization_barrier(
        (
            lax.axis_index("sp_0").astype(jnp.int32).reshape(1),
            lax.axis_index(TP).astype(jnp.int32).reshape(1),
            expert_down_weight[0],
        )
    )
    down_near = lax.ppermute(down, CORE_TP, WEIGHT_PAIRS)
    down_next = lax.ppermute(down, CORE_TP, ROW_PAIRS)

    floor = forget_minimum
    message = jax.ShapeDtypeStruct((plane, heads * piece + 16, LANES), bf16)
    states = call(
        state_kernel, message, forget_preact, value_input, floor, extra_log_decay
    )
    states = spread(states, PLANE)
    totals, before, passed = call(
        lambda *refs: plane_kernel(heads, *refs),
        (
            jax.ShapeDtypeStruct((planes, heads * piece + 16, LANES), bf16),
            jax.ShapeDtypeStruct((plane, heads * piece, LANES), f32),
            jax.ShapeDtypeStruct((plane, 8, LANES), f32),
        ),
        states,
    )
    totals = spread(totals, "sp_0")
    local = call(
        local_kernel,
        jax.ShapeDtypeStruct((3, window_rows, width), f32),
        query,
        forget_preact,
        value_input,
        output_gate,
        floor,
        extra_log_decay,
        head_norm_gain,
    )
    carried = call(
        lambda *refs: carry_kernel(heads, *refs),
        jax.ShapeDtypeStruct((plane, heads * piece, LANES), bf16),
        place,
        totals,
        before,
        passed,
        kinds="svvv",
    )
    carried = spread(carried, PLANE)
    hidden = call(
        head_kernel,
        jax.ShapeDtypeStruct((window_rows, width), bf16),
        local,
        carried,
    )
    own = lax.dynamic_slice_in_dim(routes, lax.axis_index(TP) * quarter_rows, quarter_rows, 0)
    own_rows = own.T
    tables = call(
        lambda *refs: tables_kernel(capacity, *refs),
        jax.ShapeDtypeStruct((2 * PARTS * quarter_rows, PARTS * window_rows), bf16),
        own,
        own_rows,
        router_weight,
    )
    hidden = [hidden]
    for k in range(1, tp_size):
        hidden.append(shifted(hidden[0], k))
    columns = output_weight.shape[1]
    projected = call(
        project_kernel,
        (jax.ShapeDtypeStruct((quarter_rows, columns), bf16),) * tp_size,
        tp_place,
        *hidden,
        output_weight,
        kinds="s" + "v" * (tp_size + 1),
        scratch=(pltpu.VMEM((window_rows, columns), f32),),
    )
    gate_weight, up_weight, down_near, projected = lax.optimization_barrier(
        (expert_gate_weight[0], expert_up_weight[0], down_near, projected)
    )
    mix = [projected[0]]
    for k in range(1, tp_size):
        mix.append(shifted(projected[k], k))
    down_far = lax.ppermute(down_near, CORE_TP, ROW_PAIRS)
    gate_weight_too = lax.ppermute(gate_weight, CORE_TP, WEIGHT_PAIRS)
    up_weight_too = lax.ppermute(up_weight, CORE_TP, WEIGHT_PAIRS)

    first_depth = model_width * FIRST_SHARE[0] // FIRST_SHARE[1]
    packed = [
        jax.ShapeDtypeStruct((window_rows * PARTS, depth // PARTS), bf16)
        for depth in (first_depth, model_width - first_depth)
    ]
    residual, *sends = call(
        lambda *refs: dispatch_kernel(capacity, *refs),
        (jax.ShapeDtypeStruct((quarter_rows, model_width), f32), *packed),
        tp_place,
        *mix,
        stream,
        feedforward_gain.reshape(1, -1),
        own,
        own_rows,
        kinds="s" + "v" * (tp_size + 4),
        scratch=(pltpu.VMEM((tp_size, quarter_rows, columns), bf16),),
    )
    hidden_part = expert_gate_weight.shape[2]
    rows = []
    for send in sends:
        received = spread(send.reshape(sp_size, PARTS * capacity, -1), SP).reshape(send.shape)
        rows.append((received, lax.ppermute(received, CORE_TP, ROW_PAIRS)))
    weights = (gate_weight, up_weight, gate_weight_too, up_weight_too)
    count = len(weights)
    first_rows, down_next, down_far = lax.optimization_barrier((rows[0], down_next, down_far))
    acts, kept = call(
        lambda *refs: first_kernel(capacity, *refs),
        (
            jax.ShapeDtypeStruct((2, count, window_rows, hidden_part), f32),
            jax.ShapeDtypeStruct((count, model_width - first_depth, hidden_part), bf16),
        ),
        *first_rows,
        *weights,
        mib=16,
    )
    theirs = call(
        lambda *refs: others_kernel(capacity, *refs),
        jax.ShapeDtypeStruct((window_rows, 2 * hidden_part), bf16),
        rows[1][1],
        kept,
        acts,
    )
    rest = lax.ppermute(theirs, CORE_TP, ROW_PAIRS)
    partial = call(
        lambda *refs: own_kernel(capacity, *refs),
        jax.ShapeDtypeStruct((window_rows, model_width), f32),
        rows[1][0],
        kept,
        acts,
        down,
        down_near,
        scratch=(pltpu.VMEM((window_rows, 2 * hidden_part), bf16),),
    )
    pieces = model_width // DOWN_LANES
    expert_out = call(
        lambda *refs: down_kernel(capacity, *refs),
        jax.ShapeDtypeStruct((PARTS * window_rows, model_width // PARTS), bf16),
        partial,
        rest,
        down_next,
        down_far,
        kinds="vvhh",
        scratch=(
            pltpu.VMEM((2, pieces, hidden_part, DOWN_LANES), bf16),
            pltpu.SemaphoreType.DMA((2, pieces)),
        ),
    )
    returned = spread(expert_out.reshape(sp_size, PARTS * capacity, -1), SP)
    return call(
        combine_kernel,
        jax.ShapeDtypeStruct((quarter_rows, model_width), bf16),
        returned.reshape(expert_out.shape),
        residual,
        tables,
        kinds="hvv",
        scratch=(
            pltpu.VMEM((4, expert_out.shape[0], expert_out.shape[1] // 4), bf16),
            pltpu.SemaphoreType.DMA((4,)),
        ),
    )


def solution(mesh):
    torus = Mesh(mesh.devices.reshape(8, 4, 2, 2, 2), SP_TP)
    placed = (
        P(SP, TP),
        P(SP, TP),
        P(SP, TP),
        P(SP, TP),
        P(TP),
        P(TP, SP),
        P(TP),
        P(None, TP),
        P(SP_TP, None),
        P(),
        P(SP, None),
        P(SP_TP, None),
        P(SP, None, TP),
        P(SP, None, TP),
        P(SP, TP, None),
    )
    return jax.shard_map(
        layer, mesh=torus, in_specs=placed, out_specs=P(SP_TP, None), check_vma=False
    )
```

```python
import jax
import jax.numpy as jnp
from jax import lax
from jax.experimental import pallas as pl
from jax.experimental.pallas import tpu as pltpu
from jax.sharding import Mesh
from jax.sharding import PartitionSpec as P


LANES = 128
SPAN = 64
PARTS = 2
DOWN_LANES = 512
TOPK = 2
PLANE = ("sp_1", "sp_2")
SP = ("sp_0", "sp_1", "sp_2")
TP = ("tp_0", "tp_1")
SP_TP = SP + TP
CORE_TP = ("sp_2",) + TP
EVEN_LINKS = ((0, 1), (1, 0), (2, 3), (3, 2))
ODD_LINKS = ((1, 2), (2, 1), (3, 0), (0, 3))


def by_core(first, second):
    return first + tuple((a + 4, b + 4) for a, b in second)


WEIGHT_PAIRS = by_core(EVEN_LINKS, ODD_LINKS)
ROW_PAIRS = by_core(ODD_LINKS, EVEN_LINKS)
FIRST_SHARE = (5, 6)


f32 = jnp.float32
bf16 = jnp.bfloat16
epsilon = 1e-06
exact = lax.Precision.HIGHEST


def dot(a, b, dims=((1,), (0,)), precision=None):
    return lax.dot_general(a, b, (dims, ((), ())), precision=precision, preferred_element_type=f32)


def split(value):
    high = value.astype(bf16)
    return high, (value - high.astype(f32)).astype(bf16)


def silu(value):
    return value * jax.nn.sigmoid(value)


def call(kernel, out_shape, *operands, kinds="", scratch=(), mib=12):
    spaces = {
        "v": pl.BlockSpec(memory_space=pltpu.VMEM),
        "h": pl.BlockSpec(memory_space=pltpu.HBM),
        "s": pl.BlockSpec(memory_space=pltpu.SMEM),
    }
    kinds = kinds or "v" * len(operands)
    return pl.pallas_call(
        kernel,
        out_shape=out_shape,
        in_specs=[spaces[kind] for _, kind in zip(operands, kinds, strict=True)],
        out_specs=jax.tree.map(lambda _: spaces["v"], out_shape),
        scratch_shapes=scratch,
        compiler_params=pltpu.CompilerParams(vmem_limit_bytes=mib * 1024 * 1024),
    )(*operands)


def decays(forget_ref, floor_ref, extra_ref, table):
    weight = (1.0 - floor_ref[...][None, :]) * jax.nn.sigmoid(-forget_ref[...].astype(f32))
    single = jnp.log1p(-weight)
    summed = dot(table, single, precision=exact)
    extra = extra_ref[...]
    extra_summed = dot(table, extra, ((1,), (1,)), precision=exact)
    return weight, summed, extra_summed


def state_kernel(forget_ref, value_ref, floor_ref, extra_ref, out_ref):
    rows, width = forget_ref.shape
    heads = width // LANES
    pieces = out_ref.shape[0]
    piece = LANES // pieces
    at = lax.broadcasted_iota(jnp.int32, (rows, rows), 0)
    other = lax.broadcasted_iota(jnp.int32, (rows, rows), 1)
    after = (other > at).astype(f32)
    weight, tail, extra_tail = decays(forget_ref, floor_ref, extra_ref, after)
    first = jnp.log1p(-weight[:1])
    row_at = lax.broadcasted_iota(jnp.int32, (16, LANES), 0)
    decay_rows = jnp.zeros((16, LANES), f32)
    for h in range(heads):
        lanes = slice(h * LANES, (h + 1) * LANES)
        rest = tail[:, lanes] + extra_tail[:, h : h + 1]
        total = rest[:1] + first[:, lanes] + extra_ref[h : h + 1, 0:1]
        high = total.astype(bf16).astype(f32)
        decay_rows = jnp.where(row_at == h, high, decay_rows)
        decay_rows = jnp.where(row_at == heads + h, total - high, decay_rows)
        scaled_high, scaled_low = split(weight[:, lanes] * jnp.exp(rest))
        value = value_ref[:, lanes]
        state = dot(value, scaled_high, ((0,), (0,))) + dot(value, scaled_low, ((0,), (0,)))
        for p in range(pieces):
            out_ref[p, h * piece : (h + 1) * piece, :] = state[p * piece : (p + 1) * piece].astype(bf16)
    for p in range(pieces):
        out_ref[p, heads * piece :, :] = decay_rows.astype(bf16)


def read_piece(ref, j, heads, piece):
    states = [ref[j, h * piece : (h + 1) * piece, :].astype(f32) for h in range(heads)]
    rows = ref[j, heads * piece :, :].astype(f32)
    totals = [rows[h : h + 1] + rows[heads + h : heads + h + 1] for h in range(heads)]
    return states, totals


def plane_kernel(heads, in_ref, out_ref, before_ref, passed_ref):
    members = in_ref.shape[0]
    piece = before_ref.shape[1] // heads
    running = [jnp.zeros((piece, LANES), f32) for _ in range(heads)]
    total = [jnp.zeros((1, LANES), f32) for _ in range(heads)]
    passed_ref[...] = jnp.zeros(passed_ref.shape, f32)
    for j in range(members):
        states, decay = read_piece(in_ref, j, heads, piece)
        for h in range(heads):
            before_ref[j, h * piece : (h + 1) * piece, :] = running[h]
            passed_ref[j, h : h + 1, :] = total[h]
            running[h] = jnp.exp(decay[h]) * running[h] + states[h]
            total[h] = total[h] + decay[h]
    row_at = lax.broadcasted_iota(jnp.int32, (16, LANES), 0)
    decay_rows = jnp.zeros((16, LANES), f32)
    for h in range(heads):
        high = total[h].astype(bf16).astype(f32)
        decay_rows = jnp.where(row_at == h, high, decay_rows)
        decay_rows = jnp.where(row_at == heads + h, total[h] - high, decay_rows)
    for k in range(out_ref.shape[0]):
        for h in range(heads):
            out_ref[k, h * piece : (h + 1) * piece, :] = running[h].astype(bf16)
        out_ref[k, heads * piece :, :] = decay_rows.astype(bf16)


def carry_kernel(heads, place_ref, in_ref, before_ref, passed_ref, out_ref):
    piece = before_ref.shape[1] // heads
    place = place_ref[0]
    running = [jnp.zeros((piece, LANES), f32) for _ in range(heads)]
    for k in range(in_ref.shape[0]):
        states, decay = read_piece(in_ref, k, heads, piece)
        for h in range(heads):
            following = jnp.exp(decay[h]) * running[h] + states[h]
            running[h] = jnp.where(k < place, following, running[h])
    for j in range(out_ref.shape[0]):
        for h in range(heads):
            rows = slice(h * piece, (h + 1) * piece)
            out_ref[j, rows, :] = (
                jnp.exp(passed_ref[j, h : h + 1, :]) * running[h] + before_ref[j, rows, :]
            ).astype(bf16)


def local_kernel(
    query_ref, forget_ref, value_ref, gate_ref, floor_ref, extra_ref, gain_ref, out_ref
):
    rows, width = query_ref.shape
    at = lax.broadcasted_iota(jnp.int32, (rows, rows), 0)
    other = lax.broadcasted_iota(jnp.int32, (rows, rows), 1)
    upto = ((other <= at) & (at // SPAN == other // SPAN)).astype(f32)
    weight, summed, extra_summed = decays(forget_ref, floor_ref, extra_ref, upto)
    query = silu(query_ref[...].astype(f32))
    out_ref[2] = gain_ref[...][None, :] * silu(gate_ref[...].astype(f32))
    causal = lax.broadcasted_iota(jnp.int32, (SPAN, SPAN), 0) >= lax.broadcasted_iota(
        jnp.int32, (SPAN, SPAN), 1
    )
    for h in range(width // LANES):
        lanes = slice(h * LANES, (h + 1) * LANES)
        running = summed[:, lanes] + extra_summed[:, h : h + 1]
        asked = query[:, lanes] * jnp.exp(running)
        state = jnp.zeros((LANES, LANES), f32)
        passed = jnp.zeros((1, LANES), f32)
        for b in range(rows // SPAN):
            part = slice(b * SPAN, (b + 1) * SPAN)
            decay = running[part]
            final = decay[SPAN - 1 :]
            asked_now = asked[part].astype(bf16)
            value = value_ref[part, lanes]
            given = weight[part, lanes]
            scores = dot(asked_now, (given * jnp.exp(-decay)).astype(bf16), ((1,), (1,)))
            scores = jnp.where(causal, scores, 0.0).astype(bf16)
            out = dot(scores, value)
            if b:
                out = out + dot(asked_now, state.astype(bf16), ((1,), (1,)))
            out_ref[0, part, lanes] = out
            out_ref[1, part, lanes] = asked[part] * jnp.exp(passed)
            passed = passed + final
            kept = (given * jnp.exp(final - decay)).astype(bf16)
            state = state * jnp.exp(final) + dot(value, kept, ((0,), (0,)))


def head_kernel(local_ref, carry_ref, out_ref):
    width = local_ref.shape[2]
    heads = width // LANES
    piece = carry_ref.shape[1] // heads
    for h in range(heads):
        lanes = slice(h * LANES, (h + 1) * LANES)
        carried = jnp.concatenate(
            [carry_ref[p, h * piece : (h + 1) * piece, :] for p in range(carry_ref.shape[0])], axis=0
        )
        late = local_ref[1, :, lanes].astype(bf16)
        mixed = local_ref[0, :, lanes] + dot(late, carried, ((1,), (1,)))
        scale = lax.rsqrt(jnp.mean(mixed * mixed, axis=-1, keepdims=True) + epsilon)
        out_ref[:, lanes] = (mixed * scale * local_ref[2, :, lanes]).astype(bf16)


def project_kernel(place_ref, *refs):
    count = (len(refs) - 2) // 2
    hidden_refs, (weight_ref, *out_refs, held_ref) = refs[:count], refs[count:]
    width = hidden_refs[0].shape[1]
    place = place_ref[0]
    projected = jnp.zeros(held_ref.shape, f32)
    for k, hidden_ref in enumerate(hidden_refs):
        start = pl.multiple_of((place + count - k) % count * width, width)
        projected = projected + dot(hidden_ref[...], weight_ref[pl.ds(start, width), :])
    held_ref[...] = projected
    for k, out_ref in enumerate(out_refs):
        tokens = out_ref.shape[0]
        start = pl.multiple_of((place + k) % count * tokens, tokens)
        out_ref[...] = held_ref[pl.ds(start, tokens), :].astype(bf16)


def slots_in_row(column_ref, row_ref, capacity):
    tokens = column_ref.shape[0]
    earlier = lax.broadcasted_iota(jnp.int32, (tokens, tokens), 0) < lax.broadcasted_iota(
        jnp.int32, (tokens, tokens), 1
    )
    slots = []
    for j in range(TOPK):
        mine = row_ref[j : j + 1, :]
        rank = jnp.zeros((1, tokens), f32)
        for i in range(j + 1):
            same = column_ref[:, i : i + 1] == mine
            if i == j:
                same = same & earlier
            rank = rank + jnp.sum(same.astype(f32), axis=0, keepdims=True)
        slots.append(mine * (PARTS * capacity) + rank.astype(jnp.int32))
    return slots


def slots_in_column(column_ref, row_ref, capacity):
    tokens = column_ref.shape[0]
    earlier = lax.broadcasted_iota(jnp.int32, (tokens, tokens), 1) < lax.broadcasted_iota(
        jnp.int32, (tokens, tokens), 0
    )
    slots = []
    for j in range(TOPK):
        mine = column_ref[:, j : j + 1]
        rank = jnp.zeros((tokens, 1), f32)
        for i in range(j + 1):
            same = row_ref[i : i + 1, :] == mine
            if i == j:
                same = same & earlier
            rank = rank + jnp.sum(same.astype(f32), axis=1, keepdims=True)
        slots.append(mine * (PARTS * capacity) + rank.astype(jnp.int32))
    return slots


def spread_table(rows, columns, capacity, part):
    row = lax.broadcasted_iota(jnp.int32, (rows, columns), 0)
    column = lax.broadcasted_iota(jnp.int32, (rows, columns), 1)
    stride = PARTS * capacity
    wanted = (column // capacity) * stride + part * capacity + column % capacity
    return (row == wanted).astype(f32).astype(bf16)


def gather_table(rows, columns, capacity, part):
    row = lax.broadcasted_iota(jnp.int32, (rows, columns), 0)
    column = lax.broadcasted_iota(jnp.int32, (rows, columns), 1)
    stride = PARTS * capacity
    wanted = (row // capacity) * stride + part * capacity + row % capacity
    return (column == wanted).astype(f32).astype(bf16)


def dispatch_kernel(capacity, place_ref, *refs):
    *refs, mix_ref = refs
    blocks, _, block = mix_ref.shape
    for k in range(blocks):
        mix_ref[(place_ref[0] + blocks - k) % blocks] = refs[k][...]
    stream_ref, gain_ref, column_ref, row_ref, residual_ref, *send_refs = refs[blocks:]
    tokens, width = stream_ref.shape
    square = jnp.zeros((tokens, 1), f32)
    for k in range(blocks):
        lanes = slice(k * block, (k + 1) * block)
        residual = stream_ref[:, lanes].astype(f32) + mix_ref[k].astype(f32)
        residual_ref[:, lanes] = residual
        square = square + jnp.sum(residual * residual, axis=1, keepdims=True)
    scale = lax.rsqrt(square / width + epsilon)
    slots = slots_in_row(column_ref, row_ref, capacity)
    slot_at = lax.broadcasted_iota(jnp.int32, (send_refs[0].shape[0], tokens), 0)
    tables = [
        ((slot_at == slots[0] + q * capacity) | (slot_at == slots[1] + q * capacity))
        .astype(f32)
        .astype(bf16)
        for q in range(PARTS)
    ]
    start = 0
    for send_ref in send_refs:
        part = send_ref.shape[1]
        send = jnp.zeros(send_ref.shape, f32)
        for q in range(PARTS):
            lanes = slice(start, start + part)
            start += part
            normed = (residual_ref[:, lanes] * scale * gain_ref[:, lanes]).astype(bf16)
            send = send + dot(tables[q], normed)
        send_ref[...] = send.astype(bf16)


def first_kernel(capacity, own_ref, others_ref, *refs):
    *weight_refs, acts_ref, kept_ref = refs
    depth = weight_refs[0].shape[0] - kept_ref.shape[1]
    for i, ref in enumerate((own_ref, others_ref)):
        rows = laid_out(ref, capacity)
        for j, weight_ref in enumerate(weight_refs):
            acts_ref[i, j] = dot(rows, weight_ref[:depth, :])
    for j, weight_ref in enumerate(weight_refs):
        kept_ref[j] = weight_ref[depth:, :]


def laid_out(received_ref, capacity):
    rows = received_ref.shape[0]
    tables = [gather_table(rows // PARTS, rows, capacity, q) for q in range(PARTS)]
    received = received_ref[...]
    return jnp.concatenate([dot(table, received).astype(bf16) for table in tables], axis=1)


def inner_of(rows, kept_ref, acts_ref, out_ref):
    width = kept_ref.shape[2]
    for j in range(kept_ref.shape[0] // 2):
        gate = acts_ref[2 * j] + dot(rows, kept_ref[2 * j])
        up = acts_ref[2 * j + 1] + dot(rows, kept_ref[2 * j + 1])
        out_ref[:, j * width : (j + 1) * width] = (silu(gate) * up).astype(bf16)


def others_kernel(capacity, others_ref, kept_ref, acts_ref, out_ref):
    inner_of(laid_out(others_ref, capacity), kept_ref, acts_ref.at[1], out_ref)


def own_kernel(capacity, own_ref, kept_ref, acts_ref, down_ref, near_ref, out_ref, inner_ref):
    inner_of(laid_out(own_ref, capacity), kept_ref, acts_ref.at[0], inner_ref)
    width = down_ref.shape[0]
    out_ref[...] = dot(inner_ref[:, :width], down_ref[...]) + dot(inner_ref[:, width:], near_ref[...])


def down_kernel(capacity, partial_ref, rest_ref, next_ref, far_ref, out_ref):
    rows, depth = rest_ref.shape
    block = out_ref.shape[1]
    part = next_ref.shape[1] // PARTS
    out = jnp.zeros(out_ref.shape, f32)
    for q in range(PARTS):
        lanes = pl.ds(pl.multiple_of(q * part + pl.program_id(0) * block, LANES), block)
        product = partial_ref[:, lanes] + dot(rest_ref[:, : depth // 2], next_ref[:, lanes])
        product = product + dot(rest_ref[:, depth // 2 :], far_ref[:, lanes])
        out = out + dot(spread_table(PARTS * rows, rows, capacity, q), product.astype(bf16))
    out_ref[...] = out.astype(bf16)


def project_down(capacity, partial, rest, weights):
    rows, width = partial.shape
    whole = pl.BlockSpec(memory_space=pltpu.VMEM)
    return pl.pallas_call(
        lambda *refs: down_kernel(capacity, *refs),
        grid=(width // PARTS // DOWN_LANES,),
        out_shape=jax.ShapeDtypeStruct((PARTS * rows, width // PARTS), bf16),
        in_specs=[whole, whole] + [whole for _ in weights],
        out_specs=pl.BlockSpec((PARTS * rows, DOWN_LANES), lambda k: (0, k)),
        compiler_params=pltpu.CompilerParams(vmem_limit_bytes=12 * 1024 * 1024),
    )(partial, rest, *weights)


def tables_kernel(capacity, column_ref, row_ref, weight_ref, out_ref):
    tokens = column_ref.shape[0]
    count = out_ref.shape[1]
    slots = slots_in_column(column_ref, row_ref, capacity)
    weight = weight_ref[...]
    weight = weight / jnp.sum(weight, axis=1, keepdims=True)
    for q in range(PARTS):
        slot_at = lax.broadcasted_iota(jnp.int32, (tokens, count), 1) - q * capacity
        table = jnp.zeros((tokens, count), f32)
        for j in range(TOPK):
            table = table + jnp.where(slot_at == slots[j], weight[:, j : j + 1], 0.0)
        for i, piece in enumerate(split(table)):
            out_ref[(2 * q + i) * tokens : (2 * q + i + 1) * tokens, :] = piece


def combine_kernel(results_ref, residual_ref, table_ref, out_ref, held_ref, arrived):
    pieces, _, width = held_ref.shape
    copies = [
        pltpu.make_async_copy(
            results_ref.at[:, k * width : (k + 1) * width], held_ref.at[k], arrived.at[k]
        )
        for k in range(pieces)
    ]
    for copy in copies:
        copy.start()
    tokens = residual_ref.shape[0]
    for k, copy in enumerate(copies):
        copy.wait()
        routed = dot(table_ref[...], held_ref[k])
        for q in range(PARTS):
            start = (q * pieces + k) * width
            lanes = slice(start, start + width)
            high, low = (routed[(2 * q + i) * tokens : (2 * q + i + 1) * tokens] for i in range(2))
            out_ref[:, lanes] = (residual_ref[:, lanes] + (high + low)).astype(bf16)


def spread(value, axes):
    return lax.all_to_all(value, axes, split_axis=0, concat_axis=0, tiled=True)


def shifted(value, k):
    count = lax.axis_size(TP)
    return lax.ppermute(value, TP, [(i, (i + k) % count) for i in range(count)])


def layer(
    query,
    forget_preact,
    value_input,
    output_gate,
    forget_minimum,
    extra_log_decay,
    head_norm_gain,
    output_weight,
    stream,
    feedforward_gain,
    routes,
    router_weight,
    expert_gate_weight,
    expert_up_weight,
    expert_down_weight,
):
    window_rows, width = query.shape
    heads = width // LANES
    tp_size = lax.axis_size(TP)
    sp_size = lax.axis_size(SP)
    plane = lax.axis_size(PLANE)
    planes = lax.axis_size("sp_0")
    quarter_rows, model_width = stream.shape
    capacity = window_rows // sp_size
    piece = LANES // plane

    place, tp_place, down = lax.optimization_barrier(
        (
            lax.axis_index("sp_0").astype(jnp.int32).reshape(1),
            lax.axis_index(TP).astype(jnp.int32).reshape(1),
            expert_down_weight[0],
        )
    )
    down_near = lax.ppermute(down, CORE_TP, WEIGHT_PAIRS)
    down_next = lax.ppermute(down, CORE_TP, ROW_PAIRS)

    floor = forget_minimum
    message = jax.ShapeDtypeStruct((plane, heads * piece + 16, LANES), bf16)
    states = call(
        state_kernel, message, forget_preact, value_input, floor, extra_log_decay
    )
    states = spread(states, PLANE)
    totals, before, passed = call(
        lambda *refs: plane_kernel(heads, *refs),
        (
            jax.ShapeDtypeStruct((planes, heads * piece + 16, LANES), bf16),
            jax.ShapeDtypeStruct((plane, heads * piece, LANES), f32),
            jax.ShapeDtypeStruct((plane, 8, LANES), f32),
        ),
        states,
    )
    totals = spread(totals, "sp_0")
    local = call(
        local_kernel,
        jax.ShapeDtypeStruct((3, window_rows, width), f32),
        query,
        forget_preact,
        value_input,
        output_gate,
        floor,
        extra_log_decay,
        head_norm_gain,
    )
    carried = call(
        lambda *refs: carry_kernel(heads, *refs),
        jax.ShapeDtypeStruct((plane, heads * piece, LANES), bf16),
        place,
        totals,
        before,
        passed,
        kinds="svvv",
    )
    carried = spread(carried, PLANE)
    hidden = call(
        head_kernel,
        jax.ShapeDtypeStruct((window_rows, width), bf16),
        local,
        carried,
    )
    own = lax.dynamic_slice_in_dim(routes, lax.axis_index(TP) * quarter_rows, quarter_rows, 0)
    own_rows = own.T
    tables = call(
        lambda *refs: tables_kernel(capacity, *refs),
        jax.ShapeDtypeStruct((2 * PARTS * quarter_rows, PARTS * window_rows), bf16),
        own,
        own_rows,
        router_weight,
    )
    hidden = [hidden]
    for k in range(1, tp_size):
        hidden.append(shifted(hidden[0], k))
    columns = output_weight.shape[1]
    projected = call(
        project_kernel,
        (jax.ShapeDtypeStruct((quarter_rows, columns), bf16),) * tp_size,
        tp_place,
        *hidden,
        output_weight,
        kinds="s" + "v" * (tp_size + 1),
        scratch=(pltpu.VMEM((window_rows, columns), f32),),
    )
    gate_weight, up_weight, down_near, projected = lax.optimization_barrier(
        (expert_gate_weight[0], expert_up_weight[0], down_near, projected)
    )
    mix = [projected[0]]
    for k in range(1, tp_size):
        mix.append(shifted(projected[k], k))
    down_far = lax.ppermute(down_near, CORE_TP, ROW_PAIRS)
    gate_weight_too = lax.ppermute(gate_weight, CORE_TP, WEIGHT_PAIRS)
    up_weight_too = lax.ppermute(up_weight, CORE_TP, WEIGHT_PAIRS)

    first_depth = model_width * FIRST_SHARE[0] // FIRST_SHARE[1]
    packed = [
        jax.ShapeDtypeStruct((window_rows * PARTS, depth // PARTS), bf16)
        for depth in (first_depth, model_width - first_depth)
    ]
    residual, *sends = call(
        lambda *refs: dispatch_kernel(capacity, *refs),
        (jax.ShapeDtypeStruct((quarter_rows, model_width), f32), *packed),
        tp_place,
        *mix,
        stream,
        feedforward_gain.reshape(1, -1),
        own,
        own_rows,
        kinds="s" + "v" * (tp_size + 4),
        scratch=(pltpu.VMEM((tp_size, quarter_rows, columns), bf16),),
    )
    hidden_part = expert_gate_weight.shape[2]
    rows = []
    for send in sends:
        received = spread(send.reshape(sp_size, PARTS * capacity, -1), SP).reshape(send.shape)
        rows.append((received, lax.ppermute(received, CORE_TP, ROW_PAIRS)))
    weights = (gate_weight, up_weight, gate_weight_too, up_weight_too)
    count = len(weights)
    first_rows, down_next, down_far = lax.optimization_barrier((rows[0], down_next, down_far))
    acts, kept = call(
        lambda *refs: first_kernel(capacity, *refs),
        (
            jax.ShapeDtypeStruct((2, count, window_rows, hidden_part), f32),
            jax.ShapeDtypeStruct((count, model_width - first_depth, hidden_part), bf16),
        ),
        *first_rows,
        *weights,
        mib=16,
    )
    theirs = call(
        lambda *refs: others_kernel(capacity, *refs),
        jax.ShapeDtypeStruct((window_rows, 2 * hidden_part), bf16),
        rows[1][1],
        kept,
        acts,
    )
    rest = lax.ppermute(theirs, CORE_TP, ROW_PAIRS)
    partial = call(
        lambda *refs: own_kernel(capacity, *refs),
        jax.ShapeDtypeStruct((window_rows, model_width), f32),
        rows[1][0],
        kept,
        acts,
        down,
        down_near,
        scratch=(pltpu.VMEM((window_rows, 2 * hidden_part), bf16),),
    )
    expert_out = project_down(capacity, partial, rest, (down_next, down_far))
    returned = spread(expert_out.reshape(sp_size, PARTS * capacity, -1), SP)
    return call(
        combine_kernel,
        jax.ShapeDtypeStruct((quarter_rows, model_width), bf16),
        returned.reshape(expert_out.shape),
        residual,
        tables,
        kinds="hvv",
        scratch=(
            pltpu.VMEM((4, expert_out.shape[0], expert_out.shape[1] // 4), bf16),
            pltpu.SemaphoreType.DMA((4,)),
        ),
    )


def solution(mesh):
    torus = Mesh(mesh.devices.reshape(8, 4, 2, 2, 2), SP_TP)
    placed = (
        P(SP, TP),
        P(SP, TP),
        P(SP, TP),
        P(SP, TP),
        P(TP),
        P(TP, SP),
        P(TP),
        P(None, TP),
        P(SP_TP, None),
        P(),
        P(SP, None),
        P(SP_TP, None),
        P(SP, None, TP),
        P(SP, None, TP),
        P(SP, TP, None),
    )
    return jax.shard_map(
        layer, mesh=torus, in_specs=placed, out_specs=P(SP_TP, None), check_vma=False
    )
```
